256 devices in a mesh: ep: 32 (over z, x), tp: 8 (over y, core).
Axes of the slice: x: 4, y: 4, z: 8, core: 2. Of those that a mesh axis runs over, the one named last changes fastest.
Arguments:
- tokens_first: bfloat16 [16384, 2048], P('ep'), may hold values from -6 to 6
- attn_gain: float32 [2048], replicated, may hold values from 0.1 to 1.9
- w_query: bfloat16 [2048, 1024], P(None, 'tp'), may hold values from -6 to 6
- key_matrix: bfloat16 [2048, 512], P(None, 'tp'), may hold values from -6 to 6
- value_matrix: bfloat16 [2048, 512], P(None, 'tp'), may hold values from -0.125 to 0.125
- head_sink_logit: float32 [16], P('tp'), may hold values from 1 to 5
- w_output: bfloat16 [1024, 2048], P('tp'), may hold values from -0.75 to 0.75
- tokens_second: bfloat16 [4096, 2048], P('ep'), may hold values from -6 to 6
- ffn_gain: float32 [2048], replicated, may hold values from 0.1 to 1.9
- routes: int32 [4096, 4], P('ep'), may hold values from 0 to 63, all different within a row; in each aligned block of 128 rows (0 to 127, 128 to 255, ...) at most 16 rows name the same one
- route_weight: float32 [4096, 4], P('ep'), may hold values from 0.2 to 1.5
- w_gate_exp: bfloat16 [64, 2048, 2048], P('ep', None, 'tp'), may hold values from -0.125 to 0.125
- w_up_exp: bfloat16 [64, 2048, 2048], P('ep', None, 'tp'), may hold values from -0.125 to 0.125
- w_down_exp: bfloat16 [64, 2048, 2048], P('ep', 'tp'), may hold values from -0.125 to 0.125
- w_gate_shared: bfloat16 [2048, 1024], P(None, 'tp'), may hold values from -0.125 to 0.125
- w_up_shared: bfloat16 [2048, 1024], P(None, 'tp'), may hold values from -0.125 to 0.125
- w_down_shared: bfloat16 [1024, 2048], P('tp'), may hold values from -0.1875 to 0.1875
Outputs:
- mixer_out: bfloat16 [16384, 2048], P(('ep', 'tp'))
- moe_out: bfloat16 [4096, 2048], P('ep', 'tp')
The draws below stay inside these ranges and needn't reach their ends.
Inputs may be any that keep to these rules, and one draw needn't show every extreme that they name: `routes`: each row names 4 different experts; among the rows of one index of ep no expert is named more than 16 times, a bound that some block reaches.
All inputs are finite; a program needn't handle non-finite values.
Results may differ from the reference program's by a relative error of at most 0.017.
Values may be sent and summed in bfloat16 or wider, within the bound.
A program may use at most 64 MiB of HBM per device.

```python
import math
import jax
import jax.numpy as jnp
import numpy as np
from jax import lax

MODEL_WIDTH = 2048
HEAD_SIZE = 64
QUERY_HEADS = 16
KEY_VALUE_HEADS = 8
BAND_LENGTH = 128
EFF = 2048
SFF = 1024
TOPK = 4
TOK1_DEV = 512
TOK2_DEV = 128
EXPERTS = 64
CAP = 16
TOKENS1 = 16384
TOKENS2 = 4096
N_EP = 32
N_TP = 8


def key_lookup(key):
    rotary_base = jax.random.normal(jax.random.fold_in(key, 7), (MODEL_WIDTH, KEY_VALUE_HEADS * HEAD_SIZE), jnp.float32)
    return jnp.clip(rotary_base, -6.0, 6.0) / math.sqrt(MODEL_WIDTH)


def draw_key_matrix(key, part):
    return key_lookup(key).astype(jnp.bfloat16)


def draw_w_query(key, part):
    rotary_base = jnp.clip(jax.random.normal(jax.random.fold_in(key, 11), (MODEL_WIDTH, QUERY_HEADS * HEAD_SIZE), jnp.float32), -6.0, 6.0) / math.sqrt(MODEL_WIDTH)
    return jnp.clip(rotary_base, -6.0, 6.0).astype(jnp.bfloat16)


def shard_levels(stream_key, dims, pieces, smallest, high):
    loudness = 1.0
    for position, shards_of in pieces:
        heights = jax.random.uniform(jax.random.fold_in(jax.random.fold_in(stream_key, 6), position), (shards_of,), jnp.float32, smallest / len(pieces), high / len(pieces))
        loudness = loudness * jnp.repeat(jnp.exp(heights), dims[position] // shards_of).reshape((-1,) + (1,) * (len(dims) - 1 - position))
    return loudness


def assign_block(key, own, number, rows, number_of, top, most, lean):
    ranking = jax.random.permutation(key, number_of)
    crowded, ordinary = portions_of(number_of, rows * top, most, lean, True), portions_of(number_of, rows * top, most, lean, False)
    places = jnp.arange(number_of)

    def named(tallies, offset_by):
        used = int((tallies > 0).sum())
        fixed = max(1, used // 4)
        shifted = fixed + (places - fixed + offset_by * (used - fixed)) % max(1, number_of - fixed)
        return jnp.zeros((number_of,), jnp.int32).at[ranking[jnp.where(places < fixed, places, shifted)]].set(jnp.asarray(tallies, jnp.int32))

    tallies = jnp.where(number % 4 == 0, named(crowded, number // 4), named(ordinary, number - number // 4 - 1))
    mixed = jax.random.permutation(jax.random.fold_in(own, 3), number_of)
    source_of, receiver = mixed[0:number_of // 2 * 2:2], mixed[1:number_of // 2 * 2:2]
    margin = jnp.minimum(tallies[source_of] - 1, most - tallies[receiver]) // 2
    margin = jnp.where((source_of == ranking[0]) | (receiver == ranking[0]) | (tallies[receiver] == 0), 0, jnp.maximum(margin, 0))
    shifted = jax.random.randint(jax.random.fold_in(own, 4), (number_of // 2,), 0, 1 << 20) % (margin + 1)
    tallies = tallies.at[source_of].add(-shifted).at[receiver].add(shifted)
    labels = jnp.searchsorted(jnp.cumsum(tallies), jnp.arange(rows * top), side="right").astype(jnp.int32)
    listing = labels.reshape(top, rows).T
    listing = listing[jax.random.permutation(jax.random.fold_in(own, 1), rows)]
    offset_by = jax.random.randint(jax.random.fold_in(own, 2), (rows, 1), 0, top)
    return jnp.take_along_axis(listing, (jnp.arange(top)[None, :] + offset_by) % top, axis=1)


def portions_of(number_of, total, bound, lean, full):
    portions = [(1 << 20) // math.isqrt(rank ** lean) + 1 for rank in range(1, number_of + 1)]
    largest = bound if full else min(bound, max(-(-total // number_of), total * portions[0] // sum(portions)))
    least = 1 if total - largest >= number_of - 1 else 0
    given, surplus = [largest] + [least] * (number_of - 1), total - largest - least * (number_of - 1)
    while surplus > 0:
        free = [i for i in range(1, number_of) if given[i] < largest] or [i for i in range(1, number_of) if given[i] < bound]
        mass, left = sum([portions[i] for i in free]), surplus
        for i in free:
            extra = min(bound - given[i], max(1, left * portions[i] // mass), surplus)
            given[i] = given[i] + extra
            surplus = surplus - extra
    return np.array(given)


def scatter_about(key, extent, spread, bound, pieces=(), kind=jnp.bfloat16):
    level = shard_levels(key, extent, pieces, -0.22, 0.18) if pieces else 1.0
    values = jax.random.normal(key, extent, jnp.float32) * spread * level
    return jnp.minimum(jnp.maximum(values, -bound), bound).astype(kind)


def setup_inputs(seed: int = 0) -> dict:
    arg_keys = jax.random.split(jax.random.key(seed), 18)
    tokens_first = scatter_about(arg_keys[0], (TOKENS1, MODEL_WIDTH), 1.0, 6.0, ((0, 32),))
    attn_gain = jnp.clip(1.0 + 0.18 * jax.random.normal(arg_keys[1], (MODEL_WIDTH,), jnp.float32), 0.1, 1.9)
    w_query = draw_w_query(jax.random.fold_in(arg_keys[17], 71), 0)
    key_matrix = draw_key_matrix(jax.random.fold_in(arg_keys[17], 71), 0)
    value_matrix = scatter_about(arg_keys[4], (MODEL_WIDTH, KEY_VALUE_HEADS * HEAD_SIZE), MODEL_WIDTH ** -0.5, 0.125, ((1, 8),))
    head_sink_logit = jnp.clip(1.0 + 4.0 * jax.random.uniform(arg_keys[5], (QUERY_HEADS,), jnp.float32) ** shard_levels(arg_keys[5], (QUERY_HEADS,), ((0, 8),), -0.2, 0.2), 1.0, 5.0)
    w_output = scatter_about(arg_keys[6], (QUERY_HEADS * HEAD_SIZE, MODEL_WIDTH), (QUERY_HEADS * HEAD_SIZE // 16) ** -0.5, 0.75, ((0, 8),))
    tokens_second = scatter_about(arg_keys[7], (TOKENS2, MODEL_WIDTH), 1.0, 6.0, ((0, 32),))
    ffn_gain = jnp.clip(1.0 + 0.18 * jax.random.normal(arg_keys[8], (MODEL_WIDTH,), jnp.float32), 0.1, 1.9)
    routes_keys = jax.random.split(jax.random.fold_in(arg_keys[9], 1), TOKENS2 // TOK2_DEV)
    routes_turns = jax.random.permutation(jax.random.fold_in(arg_keys[9], 3), TOKENS2 // TOK2_DEV)
    routes = jax.vmap(lambda own, number: assign_block(jax.random.fold_in(arg_keys[9], 2), own, number, TOK2_DEV, EXPERTS, TOPK, CAP, 2))(routes_keys, routes_turns).reshape((TOKENS2, TOPK))
    route_weight = jnp.clip(0.2 + 1.3 * jax.random.uniform(arg_keys[10], (TOKENS2, TOPK), jnp.float32) ** shard_levels(arg_keys[10], (TOKENS2, TOPK), ((0, 32),), -0.2, 0.2), 0.2, 1.5)
    w_gate_exp = scatter_about(arg_keys[11], (EXPERTS, MODEL_WIDTH, EFF), MODEL_WIDTH ** -0.5, 0.125, ((0, 32), (2, 8)))
    w_up_exp = scatter_about(arg_keys[12], (EXPERTS, MODEL_WIDTH, EFF), MODEL_WIDTH ** -0.5, 0.125, ((0, 32), (2, 8)))
    w_down_exp = scatter_about(arg_keys[13], (EXPERTS, EFF, MODEL_WIDTH), EFF ** -0.5, 0.125, ((0, 32), (1, 8)))
    w_gate_shared = scatter_about(arg_keys[14], (MODEL_WIDTH, SFF), MODEL_WIDTH ** -0.5, 0.125, ((1, 8),))
    w_up_shared = scatter_about(arg_keys[15], (MODEL_WIDTH, SFF), MODEL_WIDTH ** -0.5, 0.125, ((1, 8),))
    w_down_shared = scatter_about(arg_keys[16], (SFF, MODEL_WIDTH), SFF ** -0.5, 0.1875, ((0, 8),))
    return dict(tokens_first=tokens_first, attn_gain=attn_gain, w_query=w_query, key_matrix=key_matrix, value_matrix=value_matrix, head_sink_logit=head_sink_logit, w_output=w_output, tokens_second=tokens_second, ffn_gain=ffn_gain, routes=routes, route_weight=route_weight, w_gate_exp=w_gate_exp, w_up_exp=w_up_exp, w_down_exp=w_down_exp, w_gate_shared=w_gate_shared, w_up_shared=w_up_shared, w_down_shared=w_down_shared)


rope_base = 10000.0
norm_eps = 1e-06

def rms_scale(inputs, gain):
    wide = inputs.astype(jnp.float32)
    scaled = wide * lax.rsqrt(lax.optimization_barrier(jnp.mean(wide * wide, axis=-1, keepdims=True)) + norm_eps)
    return (scaled * gain).astype(jnp.bfloat16)

def apply_rotary(heads, token_positions):
    freqs = rope_base ** (-jnp.arange(0, HEAD_SIZE, 2, dtype=jnp.float32) / HEAD_SIZE)
    angles = token_positions[:, None] * freqs[None, :]
    cosine = jnp.cos(angles)[:, None, :]
    sine = jnp.sin(angles)[:, None, :]
    first_half, second_half = jnp.split(heads, 2, axis=-1)
    return jnp.concatenate([first_half * cosine - second_half * sine, second_half * cosine + first_half * sine], axis=-1)

def group_sum(rows, weights, groups):
    width = rows.shape[1] // groups
    parts = jnp.einsum('rtc,tcd->trd', rows.reshape(rows.shape[0], groups, width).astype(jnp.float32), weights.reshape(groups, width, weights.shape[1]).astype(jnp.float32))
    return lax.optimization_barrier(jnp.sum(parts.astype(jnp.bfloat16).astype(jnp.float32), axis=0))

def reference(tokens_first, attn_gain, w_query, key_matrix, value_matrix, head_sink_logit, w_output, tokens_second, ffn_gain, routes, route_weight, w_gate_exp, w_up_exp, w_down_exp, w_gate_shared, w_up_shared, w_down_shared):
    first_count = tokens_first.shape[0]
    norm_input = rms_scale(tokens_first, attn_gain)
    token_positions = jnp.arange(first_count, dtype=jnp.int32).astype(jnp.float32)
    query_rows = apply_rotary(jnp.dot(norm_input, w_query, preferred_element_type=jnp.float32).reshape(first_count, QUERY_HEADS, HEAD_SIZE), token_positions).astype(jnp.bfloat16)
    key_rows = apply_rotary(jnp.dot(norm_input, key_matrix, preferred_element_type=jnp.float32).reshape(first_count, KEY_VALUE_HEADS, HEAD_SIZE), token_positions).astype(jnp.bfloat16)
    value_rows = jnp.dot(norm_input, value_matrix, preferred_element_type=jnp.float32).astype(jnp.bfloat16).reshape(first_count, KEY_VALUE_HEADS, HEAD_SIZE)
    pad_rows = jnp.zeros((BAND_LENGTH, KEY_VALUE_HEADS, HEAD_SIZE), jnp.bfloat16)
    keys_padded = jnp.concatenate([pad_rows, key_rows], axis=0)
    values_padded = jnp.concatenate([pad_rows, value_rows], axis=0)
    layer_block = min(512, TOK1_DEV)
    head_group = QUERY_HEADS // KEY_VALUE_HEADS
    sink_scores = head_sink_logit.astype(jnp.float32).reshape(KEY_VALUE_HEADS, head_group)[:, :, None, None]

    def attend(index):
        leading_row = index * layer_block
        block_queries = lax.dynamic_slice_in_dim(query_rows, leading_row, layer_block, 0).reshape(layer_block, KEY_VALUE_HEADS, head_group, HEAD_SIZE).astype(jnp.float32)
        key_block = lax.dynamic_slice_in_dim(keys_padded, leading_row, layer_block + BAND_LENGTH, 0).astype(jnp.float32)
        value_block = lax.dynamic_slice_in_dim(values_padded, leading_row, layer_block + BAND_LENGTH, 0).astype(jnp.float32)
        scores = jnp.einsum('qhgd,khd->hgqk', block_queries, key_block) * HEAD_SIZE ** (-0.5)
        query_pos = leading_row + jnp.arange(layer_block, dtype=jnp.int32)
        key_pos = leading_row - BAND_LENGTH + jnp.arange(layer_block + BAND_LENGTH, dtype=jnp.int32)
        offsets = query_pos[:, None] - key_pos[None, :]
        visible = (offsets >= 0) & (offsets < BAND_LENGTH) & (key_pos[None, :] >= 0)
        scores = jnp.where(visible[None, None], scores, -jnp.inf)
        peak = jnp.maximum(lax.optimization_barrier(jnp.max(scores, axis=-1, keepdims=True)), sink_scores)
        expo = jnp.exp(scores - peak)
        total = lax.optimization_barrier(jnp.sum(expo, axis=-1, keepdims=True)) + jnp.exp(sink_scores - peak)
        weights = (expo / total).astype(jnp.bfloat16)
        mixed = jnp.einsum('hgqk,khd->qhgd', weights.astype(jnp.float32), value_block)
        return mixed.astype(jnp.bfloat16).reshape(layer_block, QUERY_HEADS * HEAD_SIZE)
    attended = lax.map(attend, jnp.arange(first_count // layer_block, dtype=jnp.int32)).reshape(first_count, QUERY_HEADS * HEAD_SIZE)

    def project(rows):
        return group_sum(rows, w_output, N_TP).astype(jnp.bfloat16)
    mixer_out = lax.map(project, attended.reshape(N_EP, TOK1_DEV, QUERY_HEADS * HEAD_SIZE)).reshape(first_count, MODEL_WIDTH)
    count_second = tokens_second.shape[0]
    normed_second = rms_scale(tokens_second, ffn_gain)
    flat = routes.reshape(N_EP, TOK2_DEV * TOPK)
    onehot = (flat[:, :, None] == jnp.arange(EXPERTS, dtype=jnp.int32)[None, None, :]).astype(jnp.int32)
    ranks = lax.optimization_barrier(jnp.sum((jnp.cumsum(onehot, axis=1) - onehot) * onehot, axis=-1))
    sources = jnp.arange(N_EP, dtype=jnp.int32)[:, None]
    slots = (flat * (N_EP * CAP) + sources * CAP + ranks).reshape(count_second * TOPK).astype(jnp.int32)
    row_ids = jnp.repeat(jnp.arange(count_second, dtype=jnp.int32), TOPK)
    buffer = jnp.zeros((EXPERTS * N_EP * CAP, MODEL_WIDTH), jnp.bfloat16).at[slots].set(normed_second[row_ids])

    def expert(operands):
        rows, gate_w, up_w, down_w = operands
        gate_pre = jnp.dot(rows, gate_w, preferred_element_type=jnp.float32)
        up_pre = jnp.dot(rows, up_w, preferred_element_type=jnp.float32)
        hidden = (jax.nn.silu(gate_pre) * up_pre).astype(jnp.bfloat16)
        return group_sum(hidden, down_w, N_TP).astype(jnp.bfloat16)
    results = lax.map(expert, (buffer.reshape(EXPERTS, N_EP * CAP, MODEL_WIDTH), w_gate_exp, w_up_exp, w_down_exp)).reshape(-1, MODEL_WIDTH)
    chosen = results[slots].reshape(count_second, TOPK, MODEL_WIDTH).astype(jnp.float32)
    routed = lax.optimization_barrier(jnp.sum(chosen * route_weight.astype(jnp.float32)[:, :, None], axis=1))
    shared_hidden = (jax.nn.silu(jnp.dot(normed_second, w_gate_shared, preferred_element_type=jnp.float32)) * jnp.dot(normed_second, w_up_shared, preferred_element_type=jnp.float32)).astype(jnp.bfloat16)
    shared_sum = group_sum(shared_hidden, w_down_shared, N_TP)
    moe_out = (routed + shared_sum).astype(jnp.bfloat16)
    return (mixer_out, moe_out)
```

```python
import functools

import jax
import jax.numpy as jnp
import numpy as np
from jax import lax
from jax.experimental import pallas as pl
from jax.experimental.pallas import tpu as pltpu
from jax.sharding import PartitionSpec as P

HEAD = 64
BAND = 128
CAP = 16
NX = 4
NY = 4
ROPE_BASE = 10000.0
EPS = 1e-06
MESH = pl.DeviceIdType.MESH
F32 = jnp.float32
BF16 = jnp.bfloat16


def z_order(nz):
    out = [0]
    for d in range(1, nz // 2 + 1):
        out.append(d)
        if d != nz - d:
            out.append(-d)
    return out


def rope_tables(rows, n_ep):
    freqs = ROPE_BASE ** (-np.arange(0, HEAD, 2, dtype=np.float64) / HEAD)
    lanes = np.tile(freqs, 4)[None, :]
    within = np.arange(rows, dtype=np.float64)[:, None] * lanes
    starts = np.arange(n_ep, dtype=np.float64)[:, None] * rows * lanes
    return tuple(
        np.asarray(t, np.float32) for t in (np.cos(within), np.sin(within), np.cos(starts), np.sin(starts))
    )


def kernel(cfg, *refs):
    nz, nx, n_tp, d_model, t1, t2, topk, eff, sff = cfg
    n_in = 21
    (
        tok1_h, gain1_h, wq_h, wk_h, wv_h, sink_h, wo_h, tok2_h, gain2_h, routes_h, rw_h,
        wg_h, wu_h, wd_h, sg_h, su_h, sd_h, cosb_h, sinb_h, cosa_h, sina_h,
    ) = refs[:n_in]
    mix_h, moe_h = refs[n_in : n_in + 2]
    (
        tok1, gain1, wq, wk, wv, sink, wo, tok2, gain2, routes, rw,
        wg, wu, wd, sg, su, sd, cosb, sinb, cosa, sina,
    ) = refs[n_in + 2 : 2 * n_in + 2]
    (
        n2, onehot, comb, outgoing, xs, nrm, qs, kv, wkv, pm, pmr, r2m, r1m, p_ref, pr, r2, r1, y_ref, ret, shr,
        acc, mix_o, moe_o,
        load_sem, halo_s, halo_r, dsp_s, dsp_r, ag_s, ag_r, rs_s, rs_r, mx_s, mx_r, rt_s, rt_r, st_sem,
    ) = refs[2 * n_in + 2 :]
    f = d_model // n_tp
    n_ep = nz * nx
    order = z_order(nz)
    chunks = nz // 2
    groups = p_ref.shape[3]
    slot_groups = 2 * nx
    half = (groups + 1) // 2
    s_rows = t2 // chunks

    ep = lax.axis_index("ep")
    tp = lax.axis_index("tp")
    z, x = ep // nx, ep % nx
    y, c = tp // 2, tp % 2
    partner = y * 2 + (1 - c)
    y_up, y_dn, y_far = (y + 1) % NY, (y + NY - 1) % NY, (y + 2) % NY
    up, dn, far = y_up * 2 + c, y_dn * 2 + c, y_far * 2 + c

    hbm = (tok1_h, gain1_h, wq_h, wk_h, wv_h, sink_h, wo_h, tok2_h, gain2_h, routes_h, rw_h,
           wg_h, wu_h, wd_h, sg_h, su_h, sd_h, cosb_h, sinb_h, cosa_h, sina_h)
    vmem = (tok1, gain1, wq, wk, wv, sink, wo, tok2, gain2, routes, rw,
            wg, wu, wd, sg, su, sd, cosb, sinb, cosa, sina)
    loads = [pltpu.make_async_copy(h, v, load_sem.at[i]) for i, (h, v) in enumerate(zip(hbm, vmem))]
    for i in (7, 8, 9, 10, 0, 1, 2, 3, 4, 5, 17, 18, 19, 20, 6, 14, 15, 16, 11, 12, 13):
        loads[i].start()

    barrier = pltpu.get_barrier_semaphore()
    for dz in range(nz):
        for dx in range(nx):
            if dz or dx:
                peer = ((z + dz) % nz) * nx + (x + dx) % nx
                pl.semaphore_signal(barrier, inc=1, device_id=(peer, tp), device_id_type=MESH)
    for other in (up, dn, partner):
        pl.semaphore_signal(barrier, inc=1, device_id=(ep, other), device_id_type=MESH)

    sends = []

    def send(src, dst, ssem, rsem, to_ep, to_tp):
        copy = pltpu.make_async_remote_copy(
            src_ref=src, dst_ref=dst, send_sem=ssem, recv_sem=rsem, device_id=(to_ep, to_tp), device_id_type=MESH
        )
        copy.start()
        sends.append((src, ssem))

    def arrived(dst, rsem):
        pltpu.make_async_copy(dst, dst, rsem).wait()

    for i in (7, 8, 9, 10):
        loads[i].wait()

    wide = tok2[...].astype(F32)
    scale = lax.rsqrt(jnp.mean(wide * wide, axis=-1, keepdims=True) + EPS)
    normed = (wide * scale * gain2[...]).astype(BF16)
    for j in range(n_tp):
        n2[j] = normed[:, j * f : (j + 1) * f]

    lane = lax.broadcasted_iota(jnp.int32, (t2, 128), 1)
    named = jnp.zeros((t2, 128), F32)
    weight = jnp.zeros((t2, 128), F32)
    for k in range(topk):
        hit = lane == routes[:, k : k + 1]
        named = jnp.where(hit, 1.0, named)
        weight = jnp.where(hit, rw[:, k : k + 1], weight)
    named_t = named.T
    row_i = lax.broadcasted_iota(jnp.int32, (t2, t2), 0)
    col_i = lax.broadcasted_iota(jnp.int32, (t2, t2), 1)
    before = jnp.where(row_i < col_i, 1.0, 0.0).astype(BF16)
    rank_t = jnp.dot(named_t.astype(BF16), before, preferred_element_type=F32)
    rank_t = jnp.where(named_t > 0.5, rank_t, -1.0)[: 2 * n_ep]
    cap_i = lax.broadcasted_iota(jnp.int32, (2 * n_ep, CAP, t2), 1).astype(F32)
    dispatch = jnp.where(rank_t[:, None, :] == cap_i, 1.0, 0.0).astype(BF16).reshape(2 * n_ep * CAP, t2)
    sent = jnp.dot(dispatch, n2[tp], preferred_element_type=F32).astype(BF16)
    outgoing[...] = sent.reshape(n_ep, 2, CAP, f)

    pl.semaphore_wait(barrier, n_ep - 1 + 3)

    xs[0, tp, x] = outgoing[ep]
    for p, dz in enumerate(order):
        to_z = (z + nz - dz) % nz
        for i in range(nx):
            if p == 0 and i == 0:
                continue
            to = to_z * nx + (x + i) % nx
            pltpu.make_async_remote_copy(
                src_ref=outgoing.at[to], dst_ref=xs.at[p // 2, tp, (p % 2) * nx + x], send_sem=dsp_s,
                recv_sem=dsp_r.at[p // 2], device_id=(to, tp), device_id_type=MESH,
            ).start()

    after = jnp.where(row_i > col_i, 1.0, 0.0).astype(BF16)
    rank = jnp.dot(after, named.astype(BF16), preferred_element_type=F32)
    rank = jnp.where(named > 0.5, rank, -1.0).astype(BF16)
    w_hi = weight.astype(BF16)
    w_lo = (weight - w_hi.astype(F32)).astype(BF16)
    per_z = 2 * nx * CAP
    for zz in range(nz):
        e_row = lax.broadcasted_iota(jnp.int32, (128, per_z), 0)
        e_col = lax.broadcasted_iota(jnp.int32, (128, per_z), 1)
        spread = jnp.where(e_row == zz * 2 * nx + e_col // CAP, 1.0, 0.0).astype(BF16)
        slot = (lax.broadcasted_iota(jnp.int32, (t2, per_z), 1) % CAP).astype(F32)
        mine = jnp.dot(rank, spread, preferred_element_type=F32) == slot
        comb[zz, 0] = jnp.where(mine, jnp.dot(w_hi, spread, preferred_element_type=F32), 0.0).astype(BF16)
        comb[zz, 1] = jnp.where(mine, jnp.dot(w_lo, spread, preferred_element_type=F32), 0.0).astype(BF16)

    slot_half = slot_groups // 2

    def gather_start(k):
        first = 1 if k == 0 else 0
        arrived(xs.at[k, 0, pl.ds(0, slot_groups - first)], dsp_r.at[k])
        own = xs.at[k, tp]
        send(own, own, ag_s.at[k, 0], ag_r.at[k, 0], ep, up)
        send(own, own, ag_s.at[k, 1], ag_r.at[k, 1], ep, dn)
        send(own, own, ag_s.at[k, 2], ag_r.at[k, 2], ep, partner)

    def gather_forward(k):
        low, high = pl.ds(0, slot_half), pl.ds(slot_half, slot_half)
        arrived(xs.at[k, dn], ag_r.at[k, 0])
        send(xs.at[k, dn, low], xs.at[k, dn, low], ag_s.at[k, 3], ag_r.at[k, 3], ep, up)
        send(xs.at[k, dn], xs.at[k, dn], ag_s.at[k, 5], ag_r.at[k, 5], ep, partner)
        arrived(xs.at[k, up], ag_r.at[k, 1])
        send(xs.at[k, up, high], xs.at[k, up, high], ag_s.at[k, 4], ag_r.at[k, 4], ep, dn)
        send(xs.at[k, up], xs.at[k, up], ag_s.at[k, 6], ag_r.at[k, 6], ep, partner)

    def gather_far(k):
        low, high = pl.ds(0, slot_half), pl.ds(slot_half, slot_half)
        arrived(xs.at[k, far, low], ag_r.at[k, 3])
        send(xs.at[k, far, low], xs.at[k, far, low], ag_s.at[k, 7], ag_r.at[k, 7], ep, partner)
        arrived(xs.at[k, far, high], ag_r.at[k, 4])
        send(xs.at[k, far, high], xs.at[k, far, high], ag_s.at[k, 8], ag_r.at[k, 8], ep, partner)

    def gather_end(k):
        low, high = pl.ds(0, slot_half), pl.ds(slot_half, slot_half)
        other = 1 - c
        arrived(xs.at[k, partner], ag_r.at[k, 2])
        arrived(xs.at[k, y_dn * 2 + other], ag_r.at[k, 5])
        arrived(xs.at[k, y_up * 2 + other], ag_r.at[k, 6])
        arrived(xs.at[k, y_far * 2 + other, low], ag_r.at[k, 7])
        arrived(xs.at[k, y_far * 2 + other, high], ag_r.at[k, 8])

    def pair_send(part, got, ss, rs, targets):
        for o in targets:
            t = (y + o) % NY
            send(part.at[t, 1 - c], got.at[t], ss.at[o], rs.at[o], ep, partner)

    def pair_sum(part, got, rs, o):
        t = (y + o) % NY
        arrived(got.at[t], rs.at[o])
        part[t, c] = (part[t, c].astype(F32) + got[t].astype(F32)).astype(BF16)

    def ring_first(part, got, far_in, near_in, ss, rs, h, g):
        pair_sum(part, got, rs, 2)
        pair_sum(part, got, rs, 1)
        send(part.at[y_far, c, pl.ds(0, h)], far_in.at[0, pl.ds(0, h)], ss.at[4], rs.at[4], ep, up)
        send(part.at[y_far, c, pl.ds(h, g - h)], far_in.at[1, pl.ds(0, g - h)], ss.at[5], rs.at[5], ep, dn)
        pair_sum(part, got, rs, 3)
        send(part.at[y_up, c, pl.ds(h, g - h)], near_in.at[0, pl.ds(h, g - h)], ss.at[6], rs.at[6], ep, up)
        pair_sum(part, got, rs, 0)
        send(part.at[y_dn, c, pl.ds(0, h)], near_in.at[1, pl.ds(0, h)], ss.at[7], rs.at[7], ep, dn)

    def ring_second(part, far_in, near_in, ss, rs, h, g):
        low, high = pl.ds(0, h), pl.ds(h, g - h)
        arrived(far_in.at[0, pl.ds(0, h)], rs.at[4])
        part[y_up, c, low] = (part[y_up, c, low].astype(F32) + far_in[0, pl.ds(0, h)].astype(F32)).astype(BF16)
        arrived(far_in.at[1, pl.ds(0, g - h)], rs.at[5])
        part[y_dn, c, high] = (part[y_dn, c, high].astype(F32) + far_in[1, pl.ds(0, g - h)].astype(F32)).astype(BF16)
        send(part.at[y_up, c, low], near_in.at[0, low], ss.at[8], rs.at[8], ep, up)
        send(part.at[y_dn, c, high], near_in.at[1, high], ss.at[9], rs.at[9], ep, dn)

    def ring_end(part, near_in, rs, h, g):
        low, high = pl.ds(0, h), pl.ds(h, g - h)
        arrived(near_in.at[0, high], rs.at[6])
        arrived(near_in.at[1, low], rs.at[7])
        arrived(near_in.at[0, low], rs.at[8])
        arrived(near_in.at[1, high], rs.at[9])
        return part[y, c].astype(F32) + near_in[0].astype(F32) + near_in[1].astype(F32)

    f_rows = slot_groups * CAP

    def experts(k):
        def one(e, carry):
            gate = jnp.zeros((f_rows, eff), F32)
            up_pre = jnp.zeros((f_rows, eff), F32)
            rows = jnp.concatenate([xs[k, j, :, e].reshape(f_rows, f) for j in range(n_tp)], axis=1)
            gate = jnp.dot(rows, wg[e], preferred_element_type=F32)
            up_pre = jnp.dot(rows, wu[e], preferred_element_type=F32)
            hidden = (gate / (1.0 + jnp.exp(-gate)) * up_pre).astype(BF16)
            for j in range(n_tp):
                res = jnp.dot(hidden, wd[e, :, j * f : (j + 1) * f], preferred_element_type=F32).astype(BF16)
                p_ref[k, j // 2, j % 2, pl.ds(0, slot_groups), e] = res.reshape(slot_groups, CAP, f)
            return carry

        lax.fori_loop(0, 2, one, 0)
        pair_send(p_ref.at[k], pr.at[k], rs_s.at[k], rs_r.at[k], (2, 1, 3, 0))

    def rs_first(k):
        ring_first(p_ref.at[k], pr.at[k], r2.at[k], r1.at[k], rs_s.at[k], rs_r.at[k], half, groups)

    def rs_second(k):
        ring_second(p_ref.at[k], r2.at[k], r1.at[k], rs_s.at[k], rs_r.at[k], half, groups)

    def rs_end(k):
        total = ring_end(p_ref.at[k], r1.at[k], rs_r.at[k], half, groups)
        y_ref[k] = total[:slot_groups].astype(BF16)
        shr[pl.ds(k * s_rows, s_rows)] = total[slot_groups:].reshape(s_rows, f)
        if k == 0:
            ret[z, x] = y_ref[0, x]
        for q in range(2):
            src_z = (z + nz + order[2 * k + q]) % nz
            for i in range(nx):
                if k == 0 and q == 0 and i == 0:
                    continue
                xx = (x + i) % nx
                pltpu.make_async_remote_copy(
                    src_ref=y_ref.at[k, q * nx + xx], dst_ref=ret.at[z, x], send_sem=rt_s, recv_sem=rt_r.at[k],
                    device_id=(src_z * nx + xx, tp), device_id_type=MESH,
                ).start()

    def combine(k):
        first = 1 if k == 0 else 0
        arrived(y_ref.at[k, pl.ds(0, slot_groups - first)], rt_r.at[k])
        total = jnp.zeros((t2, f), F32)
        for q in range(2):
            from_z = (z + nz - order[2 * k + q]) % nz
            rows = ret[from_z].reshape(per_z, f)
            total += jnp.dot(comb[from_z, 0], rows, preferred_element_type=F32)
            total += jnp.dot(comb[from_z, 1], rows, preferred_element_type=F32)
        if k == 0:
            acc[...] = total
        else:
            acc[...] += total

    def shared():
        for i in (14, 15, 16):
            loads[i].wait()
        rows = jnp.concatenate([n2[j] for j in range(n_tp)], axis=1)
        gate = jnp.dot(rows, sg[...], preferred_element_type=F32)
        up_pre = jnp.dot(rows, su[...], preferred_element_type=F32)
        hidden = (gate / (1.0 + jnp.exp(-gate)) * up_pre).astype(BF16)
        for j in range(n_tp):
            res = jnp.dot(hidden, sd[:, j * f : (j + 1) * f], preferred_element_type=F32).astype(BF16)
            res = res.reshape(chunks, groups - slot_groups, 2, CAP, f)
            for k in range(chunks):
                p_ref[k, j // 2, j % 2, pl.ds(slot_groups, groups - slot_groups)] = res[k]

    blk = BAND
    n_blk = t1 // blk
    lane_b = lax.broadcasted_iota(jnp.int32, (blk, 128), 1)
    low_half = (lane_b % HEAD) < HEAD // 2
    is_key = lane_b < HEAD

    def project(i, carry):
        b = (i + n_blk - 1) % n_blk
        start = pl.multiple_of(b * blk, blk)

        def norm(r, inner):
            at = pl.ds(pl.multiple_of(r * 32, 32), 32)
            rows = tok1[pl.ds(pl.multiple_of(start + r * 32, 32), 32)].astype(F32)
            scl = lax.rsqrt(jnp.mean(rows * rows, axis=-1, keepdims=True) + EPS)
            nrm[at] = (rows * scl * gain1[...]).astype(BF16)
            return inner

        lax.fori_loop(0, blk // 32, norm, 0)
        at = pl.ds(start, blk)
        ca, sa = cosa[pl.ds(ep, 1)], sina[pl.ds(ep, 1)]
        cb, sb = cosb[at], sinb[at]
        cosine = ca * cb - sa * sb
        sine = sa * cb + ca * sb
        sine = jnp.where(low_half, -sine, sine)

        def turn(v, co, si):
            other = jnp.where(low_half, pltpu.roll(v, 128 - HEAD // 2, 1), pltpu.roll(v, HEAD // 2, 1))
            return v * co + other * si

        rows = nrm[...]
        qv = jnp.dot(rows, wq[...], preferred_element_type=F32)
        qs[at] = turn(qv, cosine, sine).astype(BF16)
        kvv = jnp.dot(rows, wkv[...], preferred_element_type=F32)
        kv[pl.ds(pl.multiple_of(start + blk, blk), blk)] = turn(
            kvv, jnp.where(is_key, cosine, 1.0), jnp.where(is_key, sine, 0.0)
        ).astype(BF16)
        return carry

    def attend(b):
        keys = kv[pl.ds(b * blk, 2 * blk)]
        qb = qs[pl.ds(b * blk, blk)]
        zero = jnp.zeros_like(qb)
        q0 = jnp.where(is_key, qb, zero)
        q1 = jnp.where(is_key, pltpu.roll(qb.astype(F32), HEAD, 1).astype(BF16), zero)
        q_pos = lax.broadcasted_iota(jnp.int32, (blk, 2 * blk), 0) + blk
        k_pos = lax.broadcasted_iota(jnp.int32, (blk, 2 * blk), 1)
        gap = q_pos - k_pos
        seen = (gap >= 0) & (gap < BAND) & (k_pos + (ep * t1 + (b - 1) * blk) >= 0)
        outs = []
        for h, qh in enumerate((q0, q1)):
            s = lax.dot_general(qh, keys, (((1,), (1,)), ((), ())), preferred_element_type=F32) * HEAD**-0.5
            s = jnp.where(seen, s, -1e30)
            snk = sink[0:1, h : h + 1]
            peak = jnp.maximum(jnp.max(s, axis=-1, keepdims=True), snk)
            ex = jnp.where(seen, jnp.exp(s - peak), 0.0)
            den = jnp.sum(ex, axis=-1, keepdims=True) + jnp.exp(snk - peak)
            w = (ex / den).astype(BF16)
            outs.append(jnp.dot(w, keys, preferred_element_type=F32))
        att = jnp.where(is_key, pltpu.roll(outs[0], HEAD, 1), outs[1]).astype(BF16)
        res = jnp.dot(att, wo[...], preferred_element_type=F32).astype(BF16)
        pm[b] = res.reshape(pm.shape[1:])

    g_m = pm.shape[2]
    h_m = g_m // 2

    for i in (0, 1, 2, 3, 4, 5, 17, 18, 19, 20):
        loads[i].wait()
    wkv[...] = jnp.concatenate([wk[...], wv[...]], axis=1)
    project(0, 0)
    nxt = (ep + 1) % n_ep
    send(kv.at[pl.ds(t1, blk)], kv.at[pl.ds(0, blk)], halo_s, halo_r, nxt, tp)
    lax.fori_loop(1, n_blk, project, 0)
    gather_start(0)
    loads[6].wait()

    def attend_rest(b, carry):
        attend(b)
        return carry

    lax.fori_loop(1, n_blk, attend_rest, 0)
    gather_start(1)
    arrived(kv.at[pl.ds(0, blk)], halo_r)
    attend(0)
    pair_send(pm, pmr, mx_s, mx_r, (2, 1, 3, 0))
    gather_forward(0)
    shared()
    if chunks > 2:
        gather_start(2)
    gather_far(0)
    ring_first(pm, pmr, r2m, r1m, mx_s, mx_r, h_m, g_m)
    gather_forward(1)
    for k in range(3, chunks):
        gather_start(k)
    for i in (11, 12, 13):
        loads[i].wait()
    gather_end(0)
    experts(0)
    gather_far(1)
    ring_second(pm, r2m, r1m, mx_s, mx_r, h_m, g_m)

    def mixer_end():
        total = ring_end(pm, r1m, mx_r, h_m, g_m)
        mix_o[...] = total.astype(BF16).reshape(mix_o.shape)
        store = pltpu.make_async_copy(mix_o, mix_h, st_sem.at[0])
        store.start()
        return store

    store_mix = None
    for k in range(1, chunks):
        if k + 1 < chunks:
            gather_forward(k + 1)
        rs_first(k - 1)
        gather_end(k)
        experts(k)
        if k + 1 < chunks:
            gather_far(k + 1)
        if k == 1:
            store_mix = mixer_end()
        rs_second(k - 1)
        if k >= 2:
            rs_end(k - 2)
    rs_first(chunks - 1)
    if chunks >= 2:
        rs_end(chunks - 2)
    rs_second(chunks - 1)
    for k in range(chunks - 1):
        combine(k)
    rs_end(chunks - 1)
    combine(chunks - 1)
    moe_o[...] = (acc[...] + shr[...]).astype(BF16)
    store_moe = pltpu.make_async_copy(moe_o, moe_h, st_sem.at[1])
    store_moe.start()
    for src, sem in sends:
        pltpu.make_async_copy(src, src, sem).wait()
    whole = outgoing.at[pl.ds(0, n_ep - 1)]
    pltpu.make_async_copy(whole, whole, dsp_s).wait()
    pltpu.make_async_copy(whole, whole, rt_s).wait()
    store_mix.wait()
    store_moe.wait()


def build(mesh, nx=NX):
    n_ep = mesh.shape["ep"]
    n_tp = mesh.shape["tp"]
    nz = n_ep // nx

    def local(tok1, gain1, wq, wk, wv, sink, wo, tok2, gain2, routes, rw, wg, wu, wd, sg, su, sd):
        t1, d_model = tok1.shape
        t2, topk = routes.shape
        eff = wg.shape[2]
        sff = sg.shape[1]
        f = d_model // n_tp
        chunks = nz // 2
        slot_groups = 2 * nx
        s_groups = t2 // chunks // (2 * CAP)
        groups = slot_groups + s_groups
        half = (groups + 1) // 2
        rows_tp = t1 // n_tp
        tables = tuple(jnp.asarray(t) for t in rope_tables(t1, n_ep))
        args = (
            tok1, gain1.reshape(1, -1), wq, wk, wv, sink.reshape(1, -1), wo, tok2, gain2.reshape(1, -1), routes, rw,
            wg, wu, wd, sg, su, sd, *tables,
        )
        vm = pltpu.VMEM
        dma = pltpu.SemaphoreType.DMA
        g_m = rows_tp // 16
        scratch = [vm(a.shape, a.dtype) for a in args] + [
            vm((n_tp, t2, f), BF16),
            vm((8, 128), BF16),
            vm((nz, 2, t2, 2 * nx * CAP), BF16),
            vm((n_ep, 2, CAP, f), BF16),
            vm((chunks, n_tp, slot_groups, 2, CAP, f), BF16),
            vm((BAND, d_model), BF16),
            vm((t1, 128), BF16),
            vm((t1 + BAND, 128), BF16),
            vm((d_model, 128), BF16),
            vm((NY, 2, g_m, 16, d_model), BF16),
            vm((NY, g_m, 16, d_model), BF16),
            vm((2, g_m // 2, 16, d_model), BF16),
            vm((2, g_m, 16, d_model), BF16),
            vm((chunks, NY, 2, groups, 2, CAP, f), BF16),
            vm((chunks, NY, groups, 2, CAP, f), BF16),
            vm((chunks, 2, half, 2, CAP, f), BF16),
            vm((chunks, 2, groups, 2, CAP, f), BF16),
            vm((chunks, slot_groups, 2, CAP, f), BF16),
            vm((nz, nx, 2, CAP, f), BF16),
            vm((t2, f), F32),
            vm((t2, f), F32),
            vm((rows_tp, d_model), BF16),
            vm((t2, f), BF16),
            dma((len(args),)),
            dma, dma,
            dma, dma((chunks,)),
            dma((chunks, 9)), dma((chunks, 9)),
            dma((chunks, 10)), dma((chunks, 10)),
            dma((10,)), dma((10,)),
            dma, dma((chunks,)),
            dma((2,)),
        ]
        cfg = (nz, nx, n_tp, d_model, t1, t2, topk, eff, sff)
        return pl.pallas_call(
            functools.partial(kernel, cfg),
            name="whole",
            out_shape=(
                jax.ShapeDtypeStruct((rows_tp, d_model), BF16),
                jax.ShapeDtypeStruct((t2, f), BF16),
            ),
            in_specs=[pl.BlockSpec(memory_space=pl.ANY)] * len(args),
            out_specs=(pl.BlockSpec(memory_space=pl.ANY),) * 2,
            scratch_shapes=scratch,
            compiler_params=pltpu.CompilerParams(
                collective_id=0, has_side_effects=True, vmem_limit_bytes=60 * 1024 * 1024
            ),
        )(*args)

    in_specs = (
        P("ep", None), P(), P(None, "tp"), P(None, "tp"), P(None, "tp"), P("tp"), P("tp", None),
        P("ep", None), P(), P("ep", None), P("ep", None),
        P("ep", None, "tp"), P("ep", None, "tp"), P("ep", "tp", None),
        P(None, "tp"), P(None, "tp"), P("tp", None),
    )
    out_specs = (P(("ep", "tp"), None), P("ep", "tp"))
    return jax.shard_map(local, mesh=mesh, in_specs=in_specs, out_specs=out_specs, check_vma=False)


def solution(mesh):
    return build(mesh)
```

```python
import functools

import jax
import jax.numpy as jnp
import numpy as np
from jax import lax
from jax.experimental import pallas as pl
from jax.experimental.pallas import tpu as pltpu
from jax.sharding import PartitionSpec as P

HEAD = 64
BAND = 128
CAP = 16
NX = 4
NY = 4
ROPE_BASE = 10000.0
EPS = 1e-06
MESH = pl.DeviceIdType.MESH
F32 = jnp.float32
BF16 = jnp.bfloat16


CHUNK_Z = ((0, 1), (4, -2), (3, -3), (2,), (-1,))
SHARED = (2, 2, 0, 0, 0)
FAR_DIRECT = (0,)
SEND_ORDER = ((0, 0), (0, 1), (1, 0), (2, 0), (3, 0), (4, 0))


def rope_tables(rows, n_ep):
    freqs = ROPE_BASE ** (-np.arange(0, HEAD, 2, dtype=np.float64) / HEAD)
    lanes = np.tile(freqs, 4)[None, :]
    within = np.arange(rows, dtype=np.float64)[:, None] * lanes
    starts = np.arange(n_ep, dtype=np.float64)[:, None] * rows * lanes
    return tuple(
        np.asarray(t, np.float32) for t in (np.cos(within), np.sin(within), np.cos(starts), np.sin(starts))
    )


def kernel(cfg, *refs):
    nz, nx, n_tp, d_model, t1, t2, topk, eff, sff = cfg
    n_in = 21
    (
        tok1_h, gain1_h, wq_h, wk_h, wv_h, sink_h, wo_h, tok2_h, gain2_h, routes_h, rw_h,
        wg_h, wu_h, wd_h, sg_h, su_h, sd_h, cosb_h, sinb_h, cosa_h, sina_h,
    ) = refs[:n_in]
    mix_h, moe_h = refs[n_in : n_in + 2]
    (
        tok1, gain1, wq, wk, wv, sink, wo, tok2, gain2, routes, rw,
        wg, wu, wd, sg, su, sd, cosb, sinb, cosa, sina,
    ) = refs[n_in + 2 : 2 * n_in + 2]
    (
        n2, comb, outgoing, xs, nrm, qs, kv, wkv, wof, att, attx, p_ref, pr, r2, r1, y_ref, ret, shr,
        acc, mix_o, moe_o,
        load_sem, halo_s, halo_r, dsp_s, dsp_r, ag_s, ag_r, rs_s, rs_r, wo_s, wo_r, at_s, at_r, rt_s, rt_r, st_sem,
    ) = refs[2 * n_in + 2 :]
    f = d_model // n_tp
    n_ep = nz * nx
    chunks = len(CHUNK_Z)
    slots_of = [nx * len(c) for c in CHUNK_Z]
    groups_of = [a + b for a, b in zip(slots_of, SHARED)]
    half_of = [g // 2 for g in groups_of]
    piece = 2 * CAP
    shared_at = [piece * sum(SHARED[:k]) for k in range(chunks)]

    ep = lax.axis_index("ep")
    tp = lax.axis_index("tp")
    z, x = ep // nx, ep % nx
    y, c = tp // 2, tp % 2
    partner = y * 2 + (1 - c)
    y_up, y_dn, y_far = (y + 1) % NY, (y + NY - 1) % NY, (y + 2) % NY
    up, dn, far = y_up * 2 + c, y_dn * 2 + c, y_far * 2 + c

    hbm = (tok1_h, gain1_h, wq_h, wk_h, wv_h, sink_h, wo_h, tok2_h, gain2_h, routes_h, rw_h,
           wg_h, wu_h, wd_h, sg_h, su_h, sd_h, cosb_h, sinb_h, cosa_h, sina_h)
    vmem = (tok1, gain1, wq, wk, wv, sink, wo, tok2, gain2, routes, rw,
            wg, wu, wd, sg, su, sd, cosb, sinb, cosa, sina)
    vmem = vmem[:3] + (wkv.at[pl.ds(0, HEAD)], wkv.at[pl.ds(HEAD, HEAD)]) + vmem[5:]
    loads = [pltpu.make_async_copy(h, v, load_sem.at[i]) for i, (h, v) in enumerate(zip(hbm, vmem))]
    for i in (7, 8, 9, 10, 0, 1, 2, 3, 4, 5, 17, 18, 19, 20, 6, 14, 15, 16, 11, 12, 13):
        loads[i].start()

    barrier = pltpu.get_barrier_semaphore()
    for dz in range(nz):
        for dx in range(nx):
            if dz or dx:
                peer = ((z + dz) % nz) * nx + (x + dx) % nx
                pl.semaphore_signal(barrier, inc=1, device_id=(peer, tp), device_id_type=MESH)
    for step in range(1, n_tp):
        pl.semaphore_signal(barrier, inc=1, device_id=(ep, (tp + step) % n_tp), device_id_type=MESH)

    sends = []

    def send(src, dst, ssem, rsem, to_ep, to_tp):
        copy = pltpu.make_async_remote_copy(
            src_ref=src, dst_ref=dst, send_sem=ssem, recv_sem=rsem, device_id=(to_ep, to_tp), device_id_type=MESH
        )
        copy.start()
        sends.append((src, ssem))

    def arrived(dst, rsem):
        pltpu.make_async_copy(dst, dst, rsem).wait()

    with jax.named_scope("load_2"):
        for i in (7, 8, 9, 10):
            loads[i].wait()

    wide = tok2[...].astype(F32)
    scale = lax.rsqrt(jnp.mean(wide * wide, axis=-1, keepdims=True) + EPS)
    normed = (wide * scale * gain2[...]).astype(BF16)
    for j in range(n_tp):
        n2[j] = normed[:, j * f : (j + 1) * f]

    sub = lax.broadcasted_iota(jnp.int32, (128, t2), 0)
    named_t = jnp.zeros((128, t2), F32)
    weight_t = jnp.zeros((128, t2), F32)
    for k in range(topk):
        hit = sub == routes[k : k + 1]
        named_t = jnp.where(hit, 1.0, named_t)
        weight_t = jnp.where(hit, rw[k : k + 1], weight_t)
    row_i = lax.broadcasted_iota(jnp.int32, (t2, t2), 0)
    col_i = lax.broadcasted_iota(jnp.int32, (t2, t2), 1)
    before = jnp.where(row_i < col_i, 1.0, 0.0).astype(BF16)
    rank_t = jnp.dot(named_t.astype(BF16), before, preferred_element_type=F32)
    rank_t = jnp.where(named_t > 0.5, rank_t, -1.0)[: 2 * n_ep]
    cap_i = lax.broadcasted_iota(jnp.int32, (2 * n_ep, CAP, t2), 1).astype(F32)
    dispatch = jnp.where(rank_t[:, None, :] == cap_i, 1.0, 0.0).astype(BF16).reshape(2 * n_ep * CAP, t2)
    for far_one, column in enumerate((tp, far)):
        sent = jnp.dot(dispatch, n2[column], preferred_element_type=F32).astype(BF16)
        outgoing[far_one] = sent.reshape(n_ep, 2, CAP, f)

    def dispatch_all():
        with jax.named_scope("barrier"):
            pl.semaphore_wait(barrier, n_ep - 1 + n_tp - 1)
        send(kv.at[pl.ds(t1, BAND)], kv.at[pl.ds(0, BAND)], halo_s, halo_r, (ep + 1) % n_ep, tp)

        for far_one, column in enumerate((tp, far)):
            xs[0, column, x] = outgoing[far_one, ep]
        for k, far_one in SEND_ORDER:
            for q, dz in enumerate(CHUNK_Z[k]):
                to_z = (z + nz - dz) % nz
                for i in range(nx):
                    if dz == 0 and i == 0:
                        continue
                    to = to_z * nx + (x + i) % nx
                    pltpu.make_async_remote_copy(
                        src_ref=outgoing.at[far_one, to], dst_ref=xs.at[k, (tp, far)[far_one], q * nx + x],
                        send_sem=dsp_s, recv_sem=dsp_r.at[k, far_one], device_id=(to, tp),
                        device_id_type=MESH,
                    ).start()

    per_z = 2 * nx * CAP

    def combine_weights():
        after = jnp.where(row_i > col_i, 1.0, 0.0).astype(BF16)
        named, weight = named_t.T, weight_t.T
        rank = jnp.dot(after, named.astype(BF16), preferred_element_type=F32)
        rank = jnp.where(named > 0.5, rank, -1.0).astype(BF16)
        w_hi = weight.astype(BF16)
        w_lo = (weight - w_hi.astype(F32)).astype(BF16)
        for zz in range(nz):
            e_row = lax.broadcasted_iota(jnp.int32, (128, per_z), 0)
            e_col = lax.broadcasted_iota(jnp.int32, (128, per_z), 1)
            spread = jnp.where(e_row == zz * 2 * nx + e_col // CAP, 1.0, 0.0).astype(BF16)
            slot = (lax.broadcasted_iota(jnp.int32, (t2, per_z), 1) % CAP).astype(F32)
            mine = jnp.dot(rank, spread, preferred_element_type=F32) == slot
            comb[zz, 0] = jnp.where(mine, jnp.dot(w_hi, spread, preferred_element_type=F32), 0.0).astype(BF16)
            comb[zz, 1] = jnp.where(mine, jnp.dot(w_lo, spread, preferred_element_type=F32), 0.0).astype(BF16)

    def halves(k):
        return pl.ds(0, slots_of[k] // 2), pl.ds(slots_of[k] // 2, slots_of[k] // 2)

    def dispatched(k, far_one):
        first = 1 if k == 0 else 0
        arrived(xs.at[k, 0, pl.ds(0, slots_of[k] - first)], dsp_r.at[k, far_one])

    def gather_start(k):
        dispatched(k, 0)
        own = xs.at[k, tp, pl.ds(0, slots_of[k])]
        send(own, own, ag_s.at[k, 0], ag_r.at[k, 0], ep, up)
        send(own, own, ag_s.at[k, 1], ag_r.at[k, 1], ep, dn)
        send(own, own, ag_s.at[k, 2], ag_r.at[k, 2], ep, partner)

    def gather_forward(k):
        low, high = halves(k)
        whole = pl.ds(0, slots_of[k])
        for i, (side, part, to) in enumerate(((dn, low, up), (up, high, dn))):
            got = xs.at[k, side, whole]
            arrived(got, ag_r.at[k, i])
            if k not in FAR_DIRECT:
                on = xs.at[k, side, part]
                send(on, on, ag_s.at[k, 3 + i], ag_r.at[k, 3 + i], ep, to)
            send(got, got, ag_s.at[k, 5 + i], ag_r.at[k, 5 + i], ep, partner)

    def gather_far(k):
        if k in FAR_DIRECT:
            dispatched(k, 1)
            got = xs.at[k, far, pl.ds(0, slots_of[k])]
            send(got, got, ag_s.at[k, 7], ag_r.at[k, 7], ep, partner)
            return
        for i, part in enumerate(halves(k)):
            got = xs.at[k, far, part]
            arrived(got, ag_r.at[k, 3 + i])
            send(got, got, ag_s.at[k, 7 + i], ag_r.at[k, 7 + i], ep, partner)

    def gather_end(k):
        other = 1 - c
        whole = pl.ds(0, slots_of[k])
        arrived(xs.at[k, partner, whole], ag_r.at[k, 2])
        arrived(xs.at[k, y_dn * 2 + other, whole], ag_r.at[k, 5])
        arrived(xs.at[k, y_up * 2 + other, whole], ag_r.at[k, 6])
        if k in FAR_DIRECT:
            arrived(xs.at[k, y_far * 2 + other, whole], ag_r.at[k, 7])
            return
        for i, part in enumerate(halves(k)):
            arrived(xs.at[k, y_far * 2 + other, part], ag_r.at[k, 7 + i])

    def pair_send(part, got, ss, rs, g):
        for o in (2, 1, 3, 0):
            t = (y + o) % NY
            send(part.at[t, 1 - c, pl.ds(0, g)], got.at[t, pl.ds(0, g)], ss.at[o], rs.at[o], ep, partner)

    def pair_sum(part, got, rs, o, g):
        t = (y + o) % NY
        at = pl.ds(0, g)
        arrived(got.at[t, at], rs.at[o])
        part[t, c, at] = (part[t, c, at].astype(F32) + got[t, at].astype(F32)).astype(BF16)

    def ring_first(part, got, far_in, near_in, ss, rs, h, g):
        pair_sum(part, got, rs, 2, g)
        pair_sum(part, got, rs, 1, g)
        send(part.at[y_far, c, pl.ds(0, h)], far_in.at[0, pl.ds(0, h)], ss.at[4], rs.at[4], ep, up)
        send(part.at[y_far, c, pl.ds(h, g - h)], far_in.at[1, pl.ds(0, g - h)], ss.at[5], rs.at[5], ep, dn)
        pair_sum(part, got, rs, 3, g)
        send(part.at[y_up, c, pl.ds(h, g - h)], near_in.at[0, pl.ds(h, g - h)], ss.at[6], rs.at[6], ep, up)
        pair_sum(part, got, rs, 0, g)
        send(part.at[y_dn, c, pl.ds(0, h)], near_in.at[1, pl.ds(0, h)], ss.at[7], rs.at[7], ep, dn)

    def ring_second(part, far_in, near_in, ss, rs, h, g):
        low, high = pl.ds(0, h), pl.ds(h, g - h)
        arrived(far_in.at[0, pl.ds(0, h)], rs.at[4])
        part[y_up, c, low] = (part[y_up, c, low].astype(F32) + far_in[0, pl.ds(0, h)].astype(F32)).astype(BF16)
        arrived(far_in.at[1, pl.ds(0, g - h)], rs.at[5])
        part[y_dn, c, high] = (part[y_dn, c, high].astype(F32) + far_in[1, pl.ds(0, g - h)].astype(F32)).astype(BF16)
        send(part.at[y_up, c, low], near_in.at[0, low], ss.at[8], rs.at[8], ep, up)
        send(part.at[y_dn, c, high], near_in.at[1, high], ss.at[9], rs.at[9], ep, dn)

    def ring_end(part, near_in, rs, h, g):
        low, high = pl.ds(0, h), pl.ds(h, g - h)
        arrived(near_in.at[0, high], rs.at[6])
        arrived(near_in.at[1, low], rs.at[7])
        arrived(near_in.at[0, low], rs.at[8])
        arrived(near_in.at[1, high], rs.at[9])
        at = pl.ds(0, g)
        return part[y, c, at].astype(F32) + near_in[0, at].astype(F32) + near_in[1, at].astype(F32)

    def experts(k):
        n_slots = slots_of[k]
        at = pl.ds(0, n_slots)

        def one(e, carry):
            rows = jnp.concatenate([xs[k, j, at, e].reshape(n_slots * CAP, f) for j in range(n_tp)], axis=1)
            gate = jnp.dot(rows, wg[e], preferred_element_type=F32)
            up_pre = jnp.dot(rows, wu[e], preferred_element_type=F32)
            hidden = (gate / (1.0 + jnp.exp(-gate)) * up_pre).astype(BF16)
            for j in range(n_tp):
                res = jnp.dot(hidden, wd[e, :, j * f : (j + 1) * f], preferred_element_type=F32).astype(BF16)
                p_ref[k, j // 2, j % 2, at, e] = res.reshape(n_slots, CAP, f)
            return carry

        lax.fori_loop(0, 2, one, 0)
        pair_send(p_ref.at[k], pr.at[k], rs_s.at[k], rs_r.at[k], groups_of[k])

    def rs_first(k):
        ring_first(p_ref.at[k], pr.at[k], r2.at[k], r1.at[k], rs_s.at[k], rs_r.at[k], half_of[k], groups_of[k])

    def rs_second(k):
        ring_second(p_ref.at[k], r2.at[k], r1.at[k], rs_s.at[k], rs_r.at[k], half_of[k], groups_of[k])

    def rs_end(k):
        total = ring_end(p_ref.at[k], r1.at[k], rs_r.at[k], half_of[k], groups_of[k])
        n_slots = slots_of[k]
        y_ref[k, pl.ds(0, n_slots)] = total[:n_slots].astype(BF16)
        if SHARED[k]:
            shr[pl.ds(shared_at[k], SHARED[k] * piece)] = total[n_slots:].reshape(SHARED[k] * piece, f)
        if k == 0:
            ret[z, x] = y_ref[0, x]
        for q, dz in enumerate(CHUNK_Z[k]):
            src_z = (z + nz + dz) % nz
            for i in range(nx):
                if dz == 0 and i == 0:
                    continue
                xx = (x + i) % nx
                pltpu.make_async_remote_copy(
                    src_ref=y_ref.at[k, q * nx + xx], dst_ref=ret.at[z, x], send_sem=rt_s, recv_sem=rt_r.at[k],
                    device_id=(src_z * nx + xx, tp), device_id_type=MESH,
                ).start()

    def combine(k):
        first = 1 if k == 0 else 0
        arrived(y_ref.at[k, pl.ds(0, slots_of[k] - first)], rt_r.at[k])
        total = jnp.zeros((t2, f), F32)
        for dz in CHUNK_Z[k]:
            from_z = (z + nz - dz) % nz
            rows = ret[from_z].reshape(per_z, f)
            total += jnp.dot(comb[from_z, 0], rows, preferred_element_type=F32)
            total += jnp.dot(comb[from_z, 1], rows, preferred_element_type=F32)
        if k == 0:
            acc[...] = total
        else:
            acc[...] += total

    def shared():
        for i in (14, 15, 16):
            loads[i].wait()
        rows = jnp.concatenate([n2[j] for j in range(n_tp)], axis=1)
        gate = jnp.dot(rows, sg[...], preferred_element_type=F32)
        up_pre = jnp.dot(rows, su[...], preferred_element_type=F32)
        hidden = (gate / (1.0 + jnp.exp(-gate)) * up_pre).astype(BF16)
        for j in range(n_tp):
            res = jnp.dot(hidden, sd[:, j * f : (j + 1) * f], preferred_element_type=F32).astype(BF16)
            for k in range(chunks):
                if SHARED[k]:
                    rows_k = res[shared_at[k] : shared_at[k] + SHARED[k] * piece]
                    p_ref[k, j // 2, j % 2, pl.ds(slots_of[k], SHARED[k])] = rows_k.reshape(SHARED[k], 2, CAP, f)

    blk = BAND
    n_blk = t1 // blk
    lane_b = lax.broadcasted_iota(jnp.int32, (blk, 128), 1)
    low_half = (lane_b % HEAD) < HEAD // 2
    is_key = lane_b < HEAD

    def project(i, carry):
        b = (i + n_blk - 1) % n_blk
        start = pl.multiple_of(b * blk, blk)

        def norm(r, inner):
            at = pl.ds(pl.multiple_of(r * 32, 32), 32)
            rows = tok1[pl.ds(pl.multiple_of(start + r * 32, 32), 32)].astype(F32)
            scl = lax.rsqrt(jnp.mean(rows * rows, axis=-1, keepdims=True) + EPS)
            nrm[at] = (rows * scl * gain1[...]).astype(BF16)
            return inner

        lax.fori_loop(0, blk // 32, norm, 0)
        at = pl.ds(start, blk)
        ca, sa = cosa[pl.ds(ep, 1)], sina[pl.ds(ep, 1)]
        cb, sb = cosb[at], sinb[at]
        cosine = ca * cb - sa * sb
        sine = sa * cb + ca * sb
        sine = jnp.where(low_half, -sine, sine)

        def turn(v, co, si):
            other = jnp.where(low_half, pltpu.roll(v, 128 - HEAD // 2, 1), pltpu.roll(v, HEAD // 2, 1))
            return v * co + other * si

        rows = nrm[...]
        qv = jnp.dot(rows, wq[...], preferred_element_type=F32)
        qs[at] = turn(qv, cosine, sine).astype(BF16)
        kvv = lax.dot_general(rows, wkv[...], (((1,), (1,)), ((), ())), preferred_element_type=F32)
        kv[pl.ds(pl.multiple_of(start + blk, blk), blk)] = turn(
            kvv, jnp.where(is_key, cosine, 1.0), jnp.where(is_key, sine, 0.0)
        ).astype(BF16)
        return carry

    def attend(b):
        keys = kv[pl.ds(b * blk, 2 * blk)]
        qb = qs[pl.ds(b * blk, blk)]
        zero = jnp.zeros_like(qb)
        q0 = jnp.where(is_key, qb, zero)
        q1 = jnp.where(is_key, pltpu.roll(qb.astype(F32), HEAD, 1).astype(BF16), zero)
        q_pos = lax.broadcasted_iota(jnp.int32, (blk, 2 * blk), 0) + blk
        k_pos = lax.broadcasted_iota(jnp.int32, (blk, 2 * blk), 1)
        gap = q_pos - k_pos
        seen = (gap >= 0) & (gap < BAND) & (k_pos + (ep * t1 + (b - 1) * blk) >= 0)
        outs = []
        for h, qh in enumerate((q0, q1)):
            s = lax.dot_general(qh, keys, (((1,), (1,)), ((), ())), preferred_element_type=F32) * HEAD**-0.5
            s = jnp.where(seen, s, -1e30)
            snk = sink[0:1, h : h + 1]
            peak = jnp.maximum(jnp.max(s, axis=-1, keepdims=True), snk)
            ex = jnp.where(seen, jnp.exp(s - peak), 0.0)
            den = jnp.sum(ex, axis=-1, keepdims=True) + jnp.exp(snk - peak)
            w = (ex / den).astype(BF16)
            outs.append(jnp.dot(w, keys, preferred_element_type=F32))
        att[pl.ds(b * blk, blk)] = jnp.where(is_key, pltpu.roll(outs[0], HEAD, 1), outs[1]).astype(BF16)

    def stage(name, fn, *operands):
        with jax.named_scope(name):
            return fn(*operands)

    def wait_loads(*which):
        for i in which:
            loads[i].wait()

    def project_first():
        wait_loads(0, 1, 2, 3, 4, 5, 17, 18, 19, 20)
        lax.fori_loop(0, n_blk - 1, project, 0)

    def project_last():
        project(n_blk - 1, 0)

    def attend_rest(b, carry):
        attend(b)
        return carry

    def attend_later():
        lax.fori_loop(1, n_blk, attend_rest, 0)

    rows_tp = t1 // n_tp

    def attend_first():
        arrived(kv.at[pl.ds(0, blk)], halo_r)
        attend(0)
        for step in range(1, n_tp):
            to = (tp + step) % n_tp
            pltpu.make_async_remote_copy(
                src_ref=att.at[pl.ds(pl.multiple_of(to * rows_tp, rows_tp), rows_tp)], dst_ref=attx.at[tp],
                send_sem=at_s, recv_sem=at_r, device_id=(ep, to), device_id_type=MESH,
            ).start()
        attx[tp] = att[pl.ds(pl.multiple_of(tp * rows_tp, rows_tp), rows_tp)]

    x_up, x_dn, x_far = (x + 1) % nx, (x + nx - 1) % nx, (x + 2) % nx
    w_rows = 128 // nx
    w_half = w_rows // 2

    def weight_y_start():
        wait_loads(6)
        part = wo.at[pl.ds(pl.multiple_of(x * w_rows, w_rows), w_rows)]
        send(part, wof.at[x, c, y], wo_s.at[0], wo_r.at[0], ep, up)
        send(part, wof.at[x, c, y], wo_s.at[1], wo_r.at[1], ep, dn)
        wof[x, c, y] = wo[pl.ds(pl.multiple_of(x * w_rows, w_rows), w_rows)]

    def weight_y_forward():
        for i, (side, start, to) in enumerate(((y_dn, 0, up), (y_up, w_half, dn))):
            arrived(wof.at[x, c, side], wo_r.at[i])
            on = wof.at[x, c, side, pl.ds(start, w_half)]
            send(on, on, wo_s.at[2 + i], wo_r.at[2 + i], ep, to)

    def weight_x_start():
        for i, start in enumerate((0, w_half)):
            arrived(wof.at[x, c, y_far, pl.ds(start, w_half)], wo_r.at[2 + i])
        own = wof.at[x, c]
        send(own, own, wo_s.at[4], wo_r.at[4], z * nx + x_up, tp)
        send(own, own, wo_s.at[5], wo_r.at[5], z * nx + x_dn, tp)
        send(own, own, wo_s.at[8], wo_r.at[8], ep, partner)

    def weight_x_forward():
        for i, (side, start, to) in enumerate(((x_dn, 0, x_up), (x_up, NY // 2, x_dn))):
            got = wof.at[side, c]
            arrived(got, wo_r.at[4 + i])
            on = wof.at[side, c, pl.ds(start, NY // 2)]
            send(on, on, wo_s.at[6 + i], wo_r.at[6 + i], z * nx + to, tp)
            send(got, got, wo_s.at[9 + i], wo_r.at[9 + i], ep, partner)

    def weight_x_far():
        for i, start in enumerate((0, NY // 2)):
            got = wof.at[x_far, c, pl.ds(start, NY // 2)]
            arrived(got, wo_r.at[6 + i])
            send(got, got, wo_s.at[11 + i], wo_r.at[11 + i], ep, partner)

    def mixer_end():
        other = 1 - c
        arrived(wof.at[x, other], wo_r.at[8])
        arrived(wof.at[x_dn, other], wo_r.at[9])
        arrived(wof.at[x_up, other], wo_r.at[10])
        for i, start in enumerate((0, NY // 2)):
            arrived(wof.at[x_far, other, pl.ds(start, NY // 2)], wo_r.at[11 + i])
        arrived(attx.at[pl.ds(0, n_tp - 1)], at_r)
        rows = jnp.concatenate([attx[j] for j in range(n_tp)], axis=1)
        n_cols = 256

        def columns(n, carry):
            at = pl.ds(pl.multiple_of(n * n_cols, n_cols), n_cols)
            parts = [wof[q, j % 2, j // 2, :, at] for j in range(n_tp) for q in range(nx)]
            mix_o[:, at] = jnp.dot(rows, jnp.concatenate(parts, axis=0), preferred_element_type=F32).astype(BF16)
            return carry

        lax.fori_loop(0, d_model // n_cols, columns, 0)
        store = pltpu.make_async_copy(mix_o, mix_h, st_sem.at[0])
        store.start()
        return store

    stage("project", project_first)
    stage("dispatch", dispatch_all)
    stage("w_y_start", weight_y_start)
    stage("project_last", project_last)
    stage("attend", attend_later)
    stage("ag_start0", gather_start, 0)
    stage("w_y_fwd", weight_y_forward)
    stage("attend0", attend_first)
    stage("ag_start1", gather_start, 1)
    stage("ag_fwd0", gather_forward, 0)
    stage("shared", shared)
    stage("w_x_start", weight_x_start)
    stage("ag_far0", gather_far, 0)
    stage("ag_start2", gather_start, 2)
    stage("ag_fwd1", gather_forward, 1)
    stage("load_w", wait_loads, 11, 12, 13)
    stage("ag_end0", gather_end, 0)
    stage("experts0", experts, 0)
    stage("weights", combine_weights)
    stage("ag_start3", gather_start, 3)
    stage("ag_start4", gather_start, 4)
    stage("rs_first0", rs_first, 0)
    stage("ag_far1", gather_far, 1)
    store_mix = None
    for k in range(1, chunks):
        if k + 1 < chunks:
            stage(f"ag_fwd{k + 1}", gather_forward, k + 1)
        if k >= 2:
            stage(f"rs_first{k - 1}", rs_first, k - 1)
        stage(f"ag_end{k}", gather_end, k)
        stage(f"experts{k}", experts, k)
        if k + 1 < chunks:
            stage(f"ag_far{k + 1}", gather_far, k + 1)
        if k == 1:
            stage("w_x_fwd", weight_x_forward)
        if k == 2:
            stage("w_x_far", weight_x_far)
        stage(f"rs_second{k - 1}", rs_second, k - 1)
        if k == 3:
            store_mix = stage("mix_end", mixer_end)
        if k >= 2:
            stage(f"rs_end{k - 2}", rs_end, k - 2)
    last = chunks - 1
    stage(f"rs_first{last}", rs_first, last)
    stage(f"rs_end{last - 1}", rs_end, last - 1)
    stage(f"rs_second{last}", rs_second, last)
    stage("combine0", combine, 0)
    stage(f"rs_end{last}", rs_end, last)
    for k in range(1, chunks):
        stage(f"combine{k}", combine, k)

    def finish():
        moe_o[...] = (acc[...] + shr[...]).astype(BF16)
        store_moe = pltpu.make_async_copy(moe_o, moe_h, st_sem.at[1])
        store_moe.start()
        for src, sem in sends:
            pltpu.make_async_copy(src, src, sem).wait()
        whole = outgoing.at[0, pl.ds(0, n_ep - 1)]
        sent_far = sum(slots_of[k] for k in FAR_DIRECT) - (1 if 0 in FAR_DIRECT else 0)
        pltpu.make_async_copy(whole, whole, dsp_s).wait()
        if sent_far:
            far_part = outgoing.at[1, pl.ds(0, sent_far)]
            pltpu.make_async_copy(far_part, far_part, dsp_s).wait()
        pltpu.make_async_copy(whole, whole, rt_s).wait()
        rows_out = attx.at[pl.ds(0, n_tp - 1)]
        pltpu.make_async_copy(rows_out, rows_out, at_s).wait()
        store_mix.wait()
        store_moe.wait()

    stage("finish", finish)


def build(mesh, nx=NX):
    n_ep = mesh.shape["ep"]
    n_tp = mesh.shape["tp"]
    nz = n_ep // nx

    def local(tok1, gain1, wq, wk, wv, sink, wo, tok2, gain2, routes, rw, wg, wu, wd, sg, su, sd):
        t1, d_model = tok1.shape
        t2, topk = routes.shape
        eff = wg.shape[2]
        sff = sg.shape[1]
        f = d_model // n_tp
        chunks = len(CHUNK_Z)
        slot_groups = nx * max(len(c) for c in CHUNK_Z)
        groups = max(nx * len(c) + b for c, b in zip(CHUNK_Z, SHARED))
        half = (groups + 1) // 2
        rows_tp = t1 // n_tp
        tables = tuple(jnp.asarray(t) for t in rope_tables(t1, n_ep))
        args = (
            tok1, gain1.reshape(1, -1), wq, wk.T, wv.T, sink.reshape(1, -1), wo, tok2, gain2.reshape(1, -1), routes.T, rw.T,
            wg, wu, wd, sg, su, sd, *tables,
        )
        vm = pltpu.VMEM
        dma = pltpu.SemaphoreType.DMA
        scratch = [vm((8, 128) if i in (3, 4) else a.shape, a.dtype) for i, a in enumerate(args)] + [
            vm((n_tp, t2, f), BF16),
                vm((nz, 2, t2, 2 * nx * CAP), BF16),
            vm((2, n_ep, 2, CAP, f), BF16),
            vm((chunks, n_tp, slot_groups, 2, CAP, f), BF16),
            vm((BAND, d_model), BF16),
            vm((t1, 128), BF16),
            vm((t1 + BAND, 128), BF16),
            vm((128, d_model), BF16),
            vm((nx, 2, NY, 128 // nx, d_model), BF16),
            vm((t1, 128), BF16),
            vm((n_tp, rows_tp, 128), BF16),
            vm((chunks, NY, 2, groups, 2, CAP, f), BF16),
            vm((chunks, NY, groups, 2, CAP, f), BF16),
            vm((chunks, 2, half, 2, CAP, f), BF16),
            vm((chunks, 2, groups, 2, CAP, f), BF16),
            vm((chunks, slot_groups, 2, CAP, f), BF16),
            vm((nz, nx, 2, CAP, f), BF16),
            vm((t2, f), F32),
            vm((t2, f), F32),
            vm((rows_tp, d_model), BF16),
            vm((t2, f), BF16),
            dma((len(args),)),
            dma, dma,
            dma, dma((chunks, 2)),
            dma((chunks, 9)), dma((chunks, 9)),
            dma((chunks, 10)), dma((chunks, 10)),
            dma((13,)), dma((13,)),
            dma, dma,
            dma, dma((chunks,)),
            dma((2,)),
        ]
        cfg = (nz, nx, n_tp, d_model, t1, t2, topk, eff, sff)
        return pl.pallas_call(
            functools.partial(kernel, cfg),
            name="whole",
            out_shape=(
                jax.ShapeDtypeStruct((rows_tp, d_model), BF16),
                jax.ShapeDtypeStruct((t2, f), BF16),
            ),
            in_specs=[pl.BlockSpec(memory_space=pl.ANY)] * len(args),
            out_specs=(pl.BlockSpec(memory_space=pl.ANY),) * 2,
            scratch_shapes=scratch,
            compiler_params=pltpu.CompilerParams(
                collective_id=0, has_side_effects=True, vmem_limit_bytes=60 * 1024 * 1024
            ),
        )(*args)

    in_specs = (
        P("ep", None), P(), P(None, "tp"), P(None, "tp"), P(None, "tp"), P("tp"), P("tp", None),
        P("ep", None), P(), P("ep", None), P("ep", None),
        P("ep", None, "tp"), P("ep", None, "tp"), P("ep", "tp", None),
        P(None, "tp"), P(None, "tp"), P("tp", None),
    )
    out_specs = (P(("ep", "tp"), None), P("ep", "tp"))
    return jax.shard_map(local, mesh=mesh, in_specs=in_specs, out_specs=out_specs, check_vma=False)


def solution(mesh):
    return build(mesh)
```

```python
import functools

import jax
import jax.numpy as jnp
import numpy as np
from jax import lax
from jax.experimental import pallas as pl
from jax.experimental.pallas import tpu as pltpu
from jax.sharding import PartitionSpec as P

HEAD = 64
BAND = 128
CAP = 16
NX = 4
NY = 4
ROPE_BASE = 10000.0
EPS = 1e-06
MESH = pl.DeviceIdType.MESH
F32 = jnp.float32
BF16 = jnp.bfloat16


CHUNK_Z = ((0, 1), (4, -2), (3, -3), (2,), (-1,))
FAR_DIRECT = (2, 3, 4)
SEND_ORDER = ((0, 0), (1, 0), (2, 0), (3, 0), (4, 0), (2, 1), (3, 1), (4, 1))


def rope_tables(rows, n_ep):
    freqs = ROPE_BASE ** (-np.arange(0, HEAD, 2, dtype=np.float64) / HEAD)
    lanes = np.tile(freqs, 4)[None, :]
    within = np.arange(rows, dtype=np.float64)[:, None] * lanes
    starts = np.arange(n_ep, dtype=np.float64)[:, None] * rows * lanes
    return tuple(
        np.asarray(t, np.float32) for t in (np.cos(within), np.sin(within), np.cos(starts), np.sin(starts))
    )


def kernel(cfg, *refs):
    nz, nx, n_tp, d_model, t1, t2, topk, eff, sff = cfg
    n_in = 21
    (
        tok1_h, gain1_h, wq_h, wk_h, wv_h, sink_h, wo_h, tok2_h, gain2_h, routes_h, rw_h,
        wg_h, wu_h, wd_h, sg_h, su_h, sd_h, cosb_h, sinb_h, cosa_h, sina_h,
    ) = refs[:n_in]
    mix_o, moe_o = refs[n_in : n_in + 2]
    (
        tok1, gain1, wq, wk, wv, sink, wo, tok2, gain2, routes, rw,
        wg, wu, wd, sg, su, sd, cosb, sinb, cosa, sina,
    ) = refs[n_in + 2 : 2 * n_in + 2]
    (
        n2, comb, outgoing, xs, nrm, qs, kv, wkv, wof, att, attx, p_ref, pr, r2, r1, y_ref, ret, shr,
        acc,
        load_sem, halo_s, halo_r, dsp_s, dsp_r, ag_s, ag_r, rs_s, rs_r, wo_s, wo_r, at_s, at_r, rt_s, rt_r,
    ) = refs[2 * n_in + 2 :]
    f = d_model // n_tp
    n_ep = nz * nx
    chunks = len(CHUNK_Z)
    slots_of = [nx * len(c) for c in CHUNK_Z]
    groups_of = slots_of + [t2 // (2 * CAP)]
    half_of = [g // 2 for g in groups_of]
    home = [k for k in range(chunks) if 0 in CHUNK_Z[k]][0]
    home_q = CHUNK_Z[home].index(0)

    ep = lax.axis_index("ep")
    tp = lax.axis_index("tp")
    z, x = ep // nx, ep % nx
    y, c = tp // 2, tp % 2
    partner = y * 2 + (1 - c)
    y_up, y_dn, y_far = (y + 1) % NY, (y + NY - 1) % NY, (y + 2) % NY
    up, dn, far = y_up * 2 + c, y_dn * 2 + c, y_far * 2 + c

    hbm = (tok1_h, gain1_h, wq_h, wk_h, wv_h, sink_h, wo_h, tok2_h, gain2_h, routes_h, rw_h,
           wg_h, wu_h, wd_h, sg_h, su_h, sd_h, cosb_h, sinb_h, cosa_h, sina_h)
    vmem = (tok1, gain1, wq, wk, wv, sink, wo, tok2, gain2, routes, rw,
            wg, wu, wd, sg, su, sd, cosb, sinb, cosa, sina)
    vmem = vmem[:3] + (wkv.at[pl.ds(0, HEAD)], wkv.at[pl.ds(HEAD, HEAD)]) + vmem[5:]
    loads = [pltpu.make_async_copy(h, v, load_sem.at[i]) for i, (h, v) in enumerate(zip(hbm, vmem))]
    for i in (7, 8, 9, 10, 0, 1, 2, 3, 4, 5, 17, 18, 19, 20, 6, 14, 15, 16, 11, 12, 13):
        loads[i].start()

    barrier = pltpu.get_barrier_semaphore()
    for dz in range(nz):
        for dx in range(nx):
            if dz or dx:
                peer = ((z + dz) % nz) * nx + (x + dx) % nx
                pl.semaphore_signal(barrier, inc=1, device_id=(peer, tp), device_id_type=MESH)
    for step in range(1, n_tp):
        pl.semaphore_signal(barrier, inc=1, device_id=(ep, (tp + step) % n_tp), device_id_type=MESH)

    sends = []

    def send(src, dst, ssem, rsem, to_ep, to_tp):
        copy = pltpu.make_async_remote_copy(
            src_ref=src, dst_ref=dst, send_sem=ssem, recv_sem=rsem, device_id=(to_ep, to_tp), device_id_type=MESH
        )
        copy.start()
        sends.append((src, ssem))

    def arrived(dst, rsem):
        pltpu.make_async_copy(dst, dst, rsem).wait()

    with jax.named_scope("load_2"):
        for i in (7, 8, 9, 10):
            loads[i].wait()

    wide = tok2[...].astype(F32)
    scale = lax.rsqrt(jnp.mean(wide * wide, axis=-1, keepdims=True) + EPS)
    normed = (wide * scale * gain2[...]).astype(BF16)
    for j in range(n_tp):
        n2[j] = normed[:, j * f : (j + 1) * f]

    sub = lax.broadcasted_iota(jnp.int32, (128, t2), 0)
    named_t = jnp.zeros((128, t2), F32)
    weight_t = jnp.zeros((128, t2), F32)
    for k in range(topk):
        hit = sub == routes[k : k + 1]
        named_t = jnp.where(hit, 1.0, named_t)
        weight_t = jnp.where(hit, rw[k : k + 1], weight_t)
    row_i = lax.broadcasted_iota(jnp.int32, (t2, t2), 0)
    col_i = lax.broadcasted_iota(jnp.int32, (t2, t2), 1)
    before = jnp.where(row_i < col_i, 1.0, 0.0).astype(BF16)
    rank_t = jnp.dot(named_t.astype(BF16), before, preferred_element_type=F32)
    rank_t = jnp.where(named_t > 0.5, rank_t, -1.0)[: 2 * n_ep]
    cap_i = lax.broadcasted_iota(jnp.int32, (2 * n_ep, CAP, t2), 1).astype(F32)
    dispatch = jnp.where(rank_t[:, None, :] == cap_i, 1.0, 0.0).astype(BF16).reshape(2 * n_ep * CAP, t2)
    for far_one, column in enumerate((tp, far)):
        sent = jnp.dot(dispatch, n2[column], preferred_element_type=F32).astype(BF16)
        outgoing[far_one] = sent.reshape(n_ep, 2, CAP, f)

    def dispatch_all():
        with jax.named_scope("barrier"):
            pl.semaphore_wait(barrier, n_ep - 1 + n_tp - 1)
        send(kv.at[pl.ds(t1, BAND)], kv.at[pl.ds(0, BAND)], halo_s, halo_r, (ep + 1) % n_ep, tp)

        for far_one, column in enumerate((tp, far)):
            xs[home, column, home_q * nx + x] = outgoing[far_one, ep]
        for k, far_one in SEND_ORDER:
            for q, dz in enumerate(CHUNK_Z[k]):
                to_z = (z + nz - dz) % nz
                for i in range(nx):
                    if dz == 0 and i == 0:
                        continue
                    to = to_z * nx + (x + i) % nx
                    pltpu.make_async_remote_copy(
                        src_ref=outgoing.at[far_one, to], dst_ref=xs.at[k, (tp, far)[far_one], q * nx + x],
                        send_sem=dsp_s, recv_sem=dsp_r.at[k, far_one], device_id=(to, tp),
                        device_id_type=MESH,
                    ).start()

    per_z = 2 * nx * CAP

    def combine_weights():
        after = jnp.where(row_i > col_i, 1.0, 0.0).astype(BF16)
        named, weight = named_t.T, weight_t.T
        rank = jnp.dot(after, named.astype(BF16), preferred_element_type=F32)
        rank = jnp.where(named > 0.5, rank, -1.0).astype(BF16)
        w_hi = weight.astype(BF16)
        w_lo = (weight - w_hi.astype(F32)).astype(BF16)
        for zz in range(nz):
            e_row = lax.broadcasted_iota(jnp.int32, (128, per_z), 0)
            e_col = lax.broadcasted_iota(jnp.int32, (128, per_z), 1)
            spread = jnp.where(e_row == zz * 2 * nx + e_col // CAP, 1.0, 0.0).astype(BF16)
            slot = (lax.broadcasted_iota(jnp.int32, (t2, per_z), 1) % CAP).astype(F32)
            mine = jnp.dot(rank, spread, preferred_element_type=F32) == slot
            comb[zz, 0] = jnp.where(mine, jnp.dot(w_hi, spread, preferred_element_type=F32), 0.0).astype(BF16)
            comb[zz, 1] = jnp.where(mine, jnp.dot(w_lo, spread, preferred_element_type=F32), 0.0).astype(BF16)

    def halves(k):
        return pl.ds(0, slots_of[k] // 2), pl.ds(slots_of[k] // 2, slots_of[k] // 2)

    def dispatched(k, far_one):
        first = 1 if k == home else 0
        arrived(xs.at[k, 0, pl.ds(0, slots_of[k] - first)], dsp_r.at[k, far_one])

    def gather_start(k):
        dispatched(k, 0)
        own = xs.at[k, tp, pl.ds(0, slots_of[k])]
        send(own, own, ag_s.at[k, 0], ag_r.at[k, 0], ep, up)
        send(own, own, ag_s.at[k, 1], ag_r.at[k, 1], ep, dn)
        send(own, own, ag_s.at[k, 2], ag_r.at[k, 2], ep, partner)

    def gather_forward(k):
        low, high = halves(k)
        whole = pl.ds(0, slots_of[k])
        for i, (side, part, to) in enumerate(((dn, low, up), (up, high, dn))):
            got = xs.at[k, side, whole]
            arrived(got, ag_r.at[k, i])
            if k not in FAR_DIRECT:
                on = xs.at[k, side, part]
                send(on, on, ag_s.at[k, 3 + i], ag_r.at[k, 3 + i], ep, to)
            send(got, got, ag_s.at[k, 5 + i], ag_r.at[k, 5 + i], ep, partner)

    def gather_far(k):
        if k in FAR_DIRECT:
            dispatched(k, 1)
            got = xs.at[k, far, pl.ds(0, slots_of[k])]
            send(got, got, ag_s.at[k, 7], ag_r.at[k, 7], ep, partner)
            return
        for i, part in enumerate(halves(k)):
            got = xs.at[k, far, part]
            arrived(got, ag_r.at[k, 3 + i])
            send(got, got, ag_s.at[k, 7 + i], ag_r.at[k, 7 + i], ep, partner)

    def gather_end(k):
        other = 1 - c
        whole = pl.ds(0, slots_of[k])
        arrived(xs.at[k, partner, whole], ag_r.at[k, 2])
        arrived(xs.at[k, y_dn * 2 + other, whole], ag_r.at[k, 5])
        arrived(xs.at[k, y_up * 2 + other, whole], ag_r.at[k, 6])
        if k in FAR_DIRECT:
            arrived(xs.at[k, y_far * 2 + other, whole], ag_r.at[k, 7])
            return
        for i, part in enumerate(halves(k)):
            arrived(xs.at[k, y_far * 2 + other, part], ag_r.at[k, 7 + i])

    def pair_send(part, got, ss, rs, g):
        for o in (2, 1, 3, 0):
            t = (y + o) % NY
            send(part.at[t, 1 - c, pl.ds(0, g)], got.at[t, pl.ds(0, g)], ss.at[o], rs.at[o], ep, partner)

    def pair_sum(part, got, rs, o, g):
        t = (y + o) % NY
        at = pl.ds(0, g)
        arrived(got.at[t, at], rs.at[o])
        part[t, c, at] = (part[t, c, at].astype(F32) + got[t, at].astype(F32)).astype(BF16)

    def ring_first(part, got, far_in, near_in, ss, rs, h, g):
        pair_sum(part, got, rs, 2, g)
        pair_sum(part, got, rs, 1, g)
        send(part.at[y_far, c, pl.ds(0, h)], far_in.at[0, pl.ds(0, h)], ss.at[4], rs.at[4], ep, up)
        send(part.at[y_far, c, pl.ds(h, g - h)], far_in.at[1, pl.ds(0, g - h)], ss.at[5], rs.at[5], ep, dn)
        pair_sum(part, got, rs, 3, g)
        send(part.at[y_up, c, pl.ds(h, g - h)], near_in.at[0, pl.ds(h, g - h)], ss.at[6], rs.at[6], ep, up)
        pair_sum(part, got, rs, 0, g)
        send(part.at[y_dn, c, pl.ds(0, h)], near_in.at[1, pl.ds(0, h)], ss.at[7], rs.at[7], ep, dn)

    def ring_second(part, far_in, near_in, ss, rs, h, g):
        low, high = pl.ds(0, h), pl.ds(h, g - h)
        arrived(far_in.at[0, pl.ds(0, h)], rs.at[4])
        part[y_up, c, low] = (part[y_up, c, low].astype(F32) + far_in[0, pl.ds(0, h)].astype(F32)).astype(BF16)
        arrived(far_in.at[1, pl.ds(0, g - h)], rs.at[5])
        part[y_dn, c, high] = (part[y_dn, c, high].astype(F32) + far_in[1, pl.ds(0, g - h)].astype(F32)).astype(BF16)
        send(part.at[y_up, c, low], near_in.at[0, low], ss.at[8], rs.at[8], ep, up)
        send(part.at[y_dn, c, high], near_in.at[1, high], ss.at[9], rs.at[9], ep, dn)

    def ring_end(part, near_in, rs, h, g):
        low, high = pl.ds(0, h), pl.ds(h, g - h)
        arrived(near_in.at[0, high], rs.at[6])
        arrived(near_in.at[1, low], rs.at[7])
        arrived(near_in.at[0, low], rs.at[8])
        arrived(near_in.at[1, high], rs.at[9])
        at = pl.ds(0, g)
        return part[y, c, at].astype(F32) + near_in[0, at].astype(F32) + near_in[1, at].astype(F32)

    def experts(k):
        n_slots = slots_of[k]
        at = pl.ds(0, n_slots)

        def one(e, carry):
            rows = jnp.concatenate([xs[k, j, at, e].reshape(n_slots * CAP, f) for j in range(n_tp)], axis=1)
            gate = jnp.dot(rows, wg[e], preferred_element_type=F32)
            up_pre = jnp.dot(rows, wu[e], preferred_element_type=F32)
            hidden = (gate / (1.0 + jnp.exp(-gate)) * up_pre).astype(BF16)
            for j in range(n_tp):
                res = jnp.dot(hidden, wd[e, :, j * f : (j + 1) * f], preferred_element_type=F32).astype(BF16)
                p_ref[k, j // 2, j % 2, at, e] = res.reshape(n_slots, CAP, f)
            return carry

        lax.fori_loop(0, 2, one, 0)
        pair_send(p_ref.at[k], pr.at[k], rs_s.at[k], rs_r.at[k], groups_of[k])

    def rs_first(k):
        ring_first(p_ref.at[k], pr.at[k], r2.at[k], r1.at[k], rs_s.at[k], rs_r.at[k], half_of[k], groups_of[k])

    def rs_second(k):
        ring_second(p_ref.at[k], r2.at[k], r1.at[k], rs_s.at[k], rs_r.at[k], half_of[k], groups_of[k])

    def rs_end(k):
        total = ring_end(p_ref.at[k], r1.at[k], rs_r.at[k], half_of[k], groups_of[k])
        n_slots = slots_of[k]
        y_ref[k, pl.ds(0, n_slots)] = total.astype(BF16)
        if k == home:
            ret[z, x] = y_ref[k, home_q * nx + x]
        for q, dz in enumerate(CHUNK_Z[k]):
            src_z = (z + nz + dz) % nz
            for i in range(nx):
                if dz == 0 and i == 0:
                    continue
                xx = (x + i) % nx
                pltpu.make_async_remote_copy(
                    src_ref=y_ref.at[k, q * nx + xx], dst_ref=ret.at[z, x], send_sem=rt_s, recv_sem=rt_r.at[k],
                    device_id=(src_z * nx + xx, tp), device_id_type=MESH,
                ).start()

    def combine(k):
        first = 1 if k == home else 0
        arrived(y_ref.at[k, pl.ds(0, slots_of[k] - first)], rt_r.at[k])
        total = jnp.zeros((t2, f), F32)
        for dz in CHUNK_Z[k]:
            from_z = (z + nz - dz) % nz
            rows = ret[from_z].reshape(per_z, f)
            total += jnp.dot(comb[from_z, 0], rows, preferred_element_type=F32)
            total += jnp.dot(comb[from_z, 1], rows, preferred_element_type=F32)
        if k == 0:
            acc[...] = total
        else:
            acc[...] += total

    def shared():
        for i in (14, 15, 16):
            loads[i].wait()
        rows = jnp.concatenate([n2[j] for j in range(n_tp)], axis=1)
        gate = jnp.dot(rows, sg[...], preferred_element_type=F32)
        up_pre = jnp.dot(rows, su[...], preferred_element_type=F32)
        hidden = (gate / (1.0 + jnp.exp(-gate)) * up_pre).astype(BF16)
        for j in range(n_tp):
            res = jnp.dot(hidden, sd[:, j * f : (j + 1) * f], preferred_element_type=F32).astype(BF16)
            p_ref[chunks, j // 2, j % 2, pl.ds(0, groups_of[chunks])] = res.reshape(groups_of[chunks], 2, CAP, f)

    def shared_send():
        k = chunks
        pair_send(p_ref.at[k], pr.at[k], rs_s.at[k], rs_r.at[k], groups_of[k])

    def shared_end():
        k = chunks
        shr[...] = ring_end(p_ref.at[k], r1.at[k], rs_r.at[k], half_of[k], groups_of[k]).reshape(t2, f)

    blk = BAND
    n_blk = t1 // blk
    lane_b = lax.broadcasted_iota(jnp.int32, (blk, 128), 1)
    low_half = (lane_b % HEAD) < HEAD // 2
    is_key = lane_b < HEAD

    def project(i, carry):
        b = (i + n_blk - 1) % n_blk
        start = pl.multiple_of(b * blk, blk)

        def norm(r, inner):
            at = pl.ds(pl.multiple_of(r * 32, 32), 32)
            rows = tok1[pl.ds(pl.multiple_of(start + r * 32, 32), 32)].astype(F32)
            scl = lax.rsqrt(jnp.mean(rows * rows, axis=-1, keepdims=True) + EPS)
            nrm[at] = (rows * scl * gain1[...]).astype(BF16)
            return inner

        lax.fori_loop(0, blk // 32, norm, 0)
        at = pl.ds(start, blk)
        ca, sa = cosa[pl.ds(ep, 1)], sina[pl.ds(ep, 1)]
        cb, sb = cosb[at], sinb[at]
        cosine = ca * cb - sa * sb
        sine = sa * cb + ca * sb
        sine = jnp.where(low_half, -sine, sine)

        def turn(v, co, si):
            other = jnp.where(low_half, pltpu.roll(v, 128 - HEAD // 2, 1), pltpu.roll(v, HEAD // 2, 1))
            return v * co + other * si

        rows = nrm[...]
        qv = jnp.dot(rows, wq[...], preferred_element_type=F32)
        qs[at] = turn(qv, cosine, sine).astype(BF16)
        kvv = lax.dot_general(rows, wkv[...], (((1,), (1,)), ((), ())), preferred_element_type=F32)
        kv[pl.ds(pl.multiple_of(start + blk, blk), blk)] = turn(
            kvv, jnp.where(is_key, cosine, 1.0), jnp.where(is_key, sine, 0.0)
        ).astype(BF16)
        return carry

    def attend(b):
        keys = kv[pl.ds(b * blk, 2 * blk)]
        qb = qs[pl.ds(b * blk, blk)]
        zero = jnp.zeros_like(qb)
        q0 = jnp.where(is_key, qb, zero)
        q1 = jnp.where(is_key, pltpu.roll(qb.astype(F32), HEAD, 1).astype(BF16), zero)
        q_pos = lax.broadcasted_iota(jnp.int32, (blk, 2 * blk), 0) + blk
        k_pos = lax.broadcasted_iota(jnp.int32, (blk, 2 * blk), 1)
        gap = q_pos - k_pos
        seen = (gap >= 0) & (gap < BAND) & (k_pos + (ep * t1 + (b - 1) * blk) >= 0)
        outs = []
        for h, qh in enumerate((q0, q1)):
            s = lax.dot_general(qh, keys, (((1,), (1,)), ((), ())), preferred_element_type=F32) * HEAD**-0.5
            s = jnp.where(seen, s, -1e30)
            snk = sink[0:1, h : h + 1]
            peak = jnp.maximum(jnp.max(s, axis=-1, keepdims=True), snk)
            ex = jnp.where(seen, jnp.exp(s - peak), 0.0)
            den = jnp.sum(ex, axis=-1, keepdims=True) + jnp.exp(snk - peak)
            w = (ex / den).astype(BF16)
            outs.append(jnp.dot(w, keys, preferred_element_type=F32))
        att[pl.ds(b * blk, blk)] = jnp.where(is_key, pltpu.roll(outs[0], HEAD, 1), outs[1]).astype(BF16)

    def stage(name, fn, *operands):
        with jax.named_scope(name):
            return fn(*operands)

    def wait_loads(*which):
        for i in which:
            loads[i].wait()

    def project_first():
        wait_loads(0, 1, 2, 3, 4, 5, 17, 18, 19, 20)
        project(0, 0)

    def project_last():
        lax.fori_loop(1, n_blk, project, 0)

    def attend_rest(b, carry):
        attend(b)
        return carry

    def attend_later():
        lax.fori_loop(1, n_blk, attend_rest, 0)

    rows_tp = t1 // n_tp

    def attend_first():
        arrived(kv.at[pl.ds(0, blk)], halo_r)
        attend(0)
        for step in range(1, n_tp):
            to = (tp + step) % n_tp
            pltpu.make_async_remote_copy(
                src_ref=att.at[pl.ds(pl.multiple_of(to * rows_tp, rows_tp), rows_tp)], dst_ref=attx.at[tp],
                send_sem=at_s, recv_sem=at_r, device_id=(ep, to), device_id_type=MESH,
            ).start()
        attx[tp] = att[pl.ds(pl.multiple_of(tp * rows_tp, rows_tp), rows_tp)]

    x_up, x_dn, x_far = (x + 1) % nx, (x + nx - 1) % nx, (x + 2) % nx
    w_rows = 128 // nx
    w_half = w_rows // 2

    def weight_y_start():
        wait_loads(6)
        part = wo.at[pl.ds(pl.multiple_of(x * w_rows, w_rows), w_rows)]
        send(part, wof.at[x, c, y], wo_s.at[0], wo_r.at[0], ep, up)
        send(part, wof.at[x, c, y], wo_s.at[1], wo_r.at[1], ep, dn)
        wof[x, c, y] = wo[pl.ds(pl.multiple_of(x * w_rows, w_rows), w_rows)]

    def weight_y_forward():
        for i, (side, start, to) in enumerate(((y_dn, 0, up), (y_up, w_half, dn))):
            arrived(wof.at[x, c, side], wo_r.at[i])
            on = wof.at[x, c, side, pl.ds(start, w_half)]
            send(on, on, wo_s.at[2 + i], wo_r.at[2 + i], ep, to)

    def weight_x_start():
        for i, start in enumerate((0, w_half)):
            arrived(wof.at[x, c, y_far, pl.ds(start, w_half)], wo_r.at[2 + i])
        own = wof.at[x, c]
        send(own, own, wo_s.at[4], wo_r.at[4], z * nx + x_up, tp)
        send(own, own, wo_s.at[5], wo_r.at[5], z * nx + x_dn, tp)
        send(own, own, wo_s.at[8], wo_r.at[8], ep, partner)

    def weight_x_forward():
        for i, (side, start, to) in enumerate(((x_dn, 0, x_up), (x_up, NY // 2, x_dn))):
            got = wof.at[side, c]
            arrived(got, wo_r.at[4 + i])
            on = wof.at[side, c, pl.ds(start, NY // 2)]
            send(on, on, wo_s.at[6 + i], wo_r.at[6 + i], z * nx + to, tp)
            send(got, got, wo_s.at[9 + i], wo_r.at[9 + i], ep, partner)

    def weight_x_far():
        for i, start in enumerate((0, NY // 2)):
            got = wof.at[x_far, c, pl.ds(start, NY // 2)]
            arrived(got, wo_r.at[6 + i])
            send(got, got, wo_s.at[11 + i], wo_r.at[11 + i], ep, partner)

    def mixer_end():
        other = 1 - c
        arrived(wof.at[x, other], wo_r.at[8])
        arrived(wof.at[x_dn, other], wo_r.at[9])
        arrived(wof.at[x_up, other], wo_r.at[10])
        for i, start in enumerate((0, NY // 2)):
            arrived(wof.at[x_far, other, pl.ds(start, NY // 2)], wo_r.at[11 + i])
        arrived(attx.at[pl.ds(0, n_tp - 1)], at_r)
        rows = jnp.concatenate([attx[j] for j in range(n_tp)], axis=1)
        n_cols = 256

        def columns(n, carry):
            at = pl.ds(pl.multiple_of(n * n_cols, n_cols), n_cols)
            parts = [wof[q, j % 2, j // 2, :, at] for j in range(n_tp) for q in range(nx)]
            mix_o[:, at] = jnp.dot(rows, jnp.concatenate(parts, axis=0), preferred_element_type=F32).astype(BF16)
            return carry

        lax.fori_loop(0, d_model // n_cols, columns, 0)

    stage("project", project_first)
    stage("dispatch", dispatch_all)
    stage("w_y_start", weight_y_start)
    stage("project_last", project_last)
    stage("ag_start0", gather_start, 0)
    stage("shared", shared)
    stage("shared_send", shared_send)
    stage("w_y_fwd", weight_y_forward)
    stage("attend", attend_later)
    stage("ag_start1", gather_start, 1)
    stage("ag_fwd0", gather_forward, 0)
    stage("shared_first", rs_first, chunks)
    stage("ag_start2", gather_start, 2)
    stage("attend0", attend_first)
    stage("ag_far0", gather_far, 0)
    stage("shared_second", rs_second, chunks)
    stage("w_x_start", weight_x_start)
    stage("ag_fwd1", gather_forward, 1)
    stage("load_w", wait_loads, 11, 12, 13)
    stage("ag_end0", gather_end, 0)
    stage("experts0", experts, 0)
    stage("ag_start3", gather_start, 3)
    stage("ag_start4", gather_start, 4)
    stage("ag_far1", gather_far, 1)
    stage("ag_fwd2", gather_forward, 2)
    stage("rs_first0", rs_first, 0)
    stage("ag_end1", gather_end, 1)
    stage("experts1", experts, 1)
    stage("ag_fwd3", gather_forward, 3)
    stage("ag_fwd4", gather_forward, 4)
    stage("ag_far2", gather_far, 2)
    stage("weights", combine_weights)
    stage("rs_first1", rs_first, 1)
    stage("rs_second0", rs_second, 0)
    stage("ag_end2", gather_end, 2)
    stage("experts2", experts, 2)
    stage("w_x_fwd", weight_x_forward)
    stage("ag_far3", gather_far, 3)
    stage("ag_far4", gather_far, 4)
    stage("ag_end3", gather_end, 3)
    stage("experts3", experts, 3)
    stage("rs_first2", rs_first, 2)
    stage("rs_second1", rs_second, 1)
    stage("rs_end0", rs_end, 0)
    stage("ag_end4", gather_end, 4)
    stage("experts4", experts, 4)
    stage("shared_end", shared_end)
    stage("rs_first3", rs_first, 3)
    stage("rs_first4", rs_first, 4)
    stage("rs_second2", rs_second, 2)
    stage("rs_end1", rs_end, 1)
    stage("rs_second3", rs_second, 3)
    stage("rs_second4", rs_second, 4)
    stage("rs_end2", rs_end, 2)
    stage("w_x_far", weight_x_far)
    stage("rs_end3", rs_end, 3)
    stage("rs_end4", rs_end, 4)
    stage("mix_end", mixer_end)
    for k in range(chunks):
        stage(f"combine{k}", combine, k)

    def finish():
        moe_o[...] = (acc[...] + shr[...]).astype(BF16)
        for src, sem in sends:
            pltpu.make_async_copy(src, src, sem).wait()
        whole = outgoing.at[0, pl.ds(0, n_ep - 1)]
        sent_far = sum(slots_of[k] for k in FAR_DIRECT) - (1 if home in FAR_DIRECT else 0)
        pltpu.make_async_copy(whole, whole, dsp_s).wait()
        if sent_far:
            far_part = outgoing.at[1, pl.ds(0, sent_far)]
            pltpu.make_async_copy(far_part, far_part, dsp_s).wait()
        pltpu.make_async_copy(whole, whole, rt_s).wait()
        rows_out = attx.at[pl.ds(0, n_tp - 1)]
        pltpu.make_async_copy(rows_out, rows_out, at_s).wait()

    stage("finish", finish)


def build(mesh, nx=NX):
    n_ep = mesh.shape["ep"]
    n_tp = mesh.shape["tp"]
    nz = n_ep // nx

    def local(tok1, gain1, wq, wk, wv, sink, wo, tok2, gain2, routes, rw, wg, wu, wd, sg, su, sd):
        t1, d_model = tok1.shape
        t2, topk = routes.shape
        eff = wg.shape[2]
        sff = sg.shape[1]
        f = d_model // n_tp
        chunks = len(CHUNK_Z)
        slot_groups = nx * max(len(c) for c in CHUNK_Z)
        groups = max(slot_groups, t2 // (2 * CAP))
        half = (groups + 1) // 2
        rows_tp = t1 // n_tp
        tables = tuple(jnp.asarray(t) for t in rope_tables(t1, n_ep))
        args = (
            tok1, gain1.reshape(1, -1), wq, wk.T, wv.T, sink.reshape(1, -1), wo, tok2, gain2.reshape(1, -1), routes.T, rw.T,
            wg, wu, wd, sg, su, sd, *tables,
        )
        vm = pltpu.VMEM
        dma = pltpu.SemaphoreType.DMA
        scratch = [vm((8, 128) if i in (3, 4) else a.shape, a.dtype) for i, a in enumerate(args)] + [
            vm((n_tp, t2, f), BF16),
                vm((nz, 2, t2, 2 * nx * CAP), BF16),
            vm((2, n_ep, 2, CAP, f), BF16),
            vm((chunks, n_tp, slot_groups, 2, CAP, f), BF16),
            vm((BAND, d_model), BF16),
            vm((t1, 128), BF16),
            vm((t1 + BAND, 128), BF16),
            vm((128, d_model), BF16),
            vm((nx, 2, NY, 128 // nx, d_model), BF16),
            vm((t1, 128), BF16),
            vm((n_tp, rows_tp, 128), BF16),
            vm((chunks + 1, NY, 2, groups, 2, CAP, f), BF16),
            vm((chunks + 1, NY, groups, 2, CAP, f), BF16),
            vm((chunks + 1, 2, half, 2, CAP, f), BF16),
            vm((chunks + 1, 2, groups, 2, CAP, f), BF16),
            vm((chunks, slot_groups, 2, CAP, f), BF16),
            vm((nz, nx, 2, CAP, f), BF16),
            vm((t2, f), F32),
            vm((t2, f), F32),
            dma((len(args),)),
            dma, dma,
            dma, dma((chunks, 2)),
            dma((chunks, 9)), dma((chunks, 9)),
            dma((chunks + 1, 10)), dma((chunks + 1, 10)),
            dma((13,)), dma((13,)),
            dma, dma,
            dma, dma((chunks,)),
        ]
        cfg = (nz, nx, n_tp, d_model, t1, t2, topk, eff, sff)
        return pl.pallas_call(
            functools.partial(kernel, cfg),
            name="whole",
            out_shape=(
                jax.ShapeDtypeStruct((rows_tp, d_model), BF16),
                jax.ShapeDtypeStruct((t2, f), BF16),
            ),
            in_specs=[pl.BlockSpec(memory_space=pltpu.HBM)] * len(args),
            out_specs=(pl.BlockSpec(memory_space=pltpu.VMEM),) * 2,
            scratch_shapes=scratch,
            compiler_params=pltpu.CompilerParams(
                collective_id=0, has_side_effects=True, vmem_limit_bytes=44 * 1024 * 1024
            ),
        )(*[pltpu.with_memory_space_constraint(a, pltpu.HBM) for a in args])
    in_specs = (
        P("ep", None), P(), P(None, "tp"), P(None, "tp"), P(None, "tp"), P("tp"), P("tp", None),
        P("ep", None), P(), P("ep", None), P("ep", None),
        P("ep", None, "tp"), P("ep", None, "tp"), P("ep", "tp", None),
        P(None, "tp"), P(None, "tp"), P("tp", None),
    )
    out_specs = (P(("ep", "tp"), None), P("ep", "tp"))
    return jax.shard_map(local, mesh=mesh, in_specs=in_specs, out_specs=out_specs, check_vma=False)


def solution(mesh):
    return build(mesh)
```

```python
import functools

import jax
import jax.numpy as jnp
import numpy as np
from jax import lax
from jax.experimental import pallas as pl
from jax.experimental.pallas import tpu as pltpu
from jax.sharding import PartitionSpec as P

HEAD = 64
BAND = 128
CAP = 16
NX = 4
NY = 4
ROPE_BASE = 10000.0
EPS = 1e-06
MESH = pl.DeviceIdType.MESH
F32 = jnp.float32
BF16 = jnp.bfloat16


CHUNK_Z = ((0, 1), (4, -2), (3, -3), (2,), (-1,))
FAR_DIRECT = (0, 2, 3, 4)
SEND_ORDER = ((0, 0), (0, 1), (1, 0), (2, 0), (3, 0), (4, 0), (2, 1), (3, 1), (4, 1))


def rope_tables(rows, n_ep):
    freqs = ROPE_BASE ** (-np.arange(0, HEAD, 2, dtype=np.float64) / HEAD)
    lanes = np.tile(freqs, 4)[None, :]
    within = np.arange(rows, dtype=np.float64)[:, None] * lanes
    starts = np.arange(n_ep, dtype=np.float64)[:, None] * rows * lanes
    return tuple(
        np.asarray(t, np.float32) for t in (np.cos(within), np.sin(within), np.cos(starts), np.sin(starts))
    )


def kernel(cfg, *refs):
    nz, nx, n_tp, d_model, t1, t2, topk, eff, sff = cfg
    n_in = 21
    (
        tok1_h, gain1_h, wq_h, wk_h, wv_h, sink_h, wo_h, tok2_h, gain2_h, routes_h, rw_h,
        wg_h, wu_h, wd_h, sg_h, su_h, sd_h, cosb_h, sinb_h, cosa_h, sina_h,
    ) = refs[:n_in]
    mix_o, moe_o = refs[n_in : n_in + 2]
    (
        tok1, gain1, wq, wk, wv, sink, wo, tok2, gain2, routes, rw,
        wg, wu, wd, sg, su, sd, cosb, sinb, cosa, sina,
    ) = refs[n_in + 2 : 2 * n_in + 2]
    (
        n2, comb, outgoing, xs, nrm, qs, kv, wkv, wof, att, attx, p_ref, pr, r2, r1, y_ref, ret, shr,
        acc,
        load_sem, halo_s, halo_r, dsp_s, dsp_r, ag_s, ag_r, rs_s, rs_r, wo_s, wo_r, at_s, at_r, rt_s, rt_r,
    ) = refs[2 * n_in + 2 :]
    f = d_model // n_tp
    n_ep = nz * nx
    chunks = len(CHUNK_Z)
    slots_of = [nx * len(c) for c in CHUNK_Z]
    groups_of = slots_of + [t2 // (2 * CAP)]
    half_of = [g // 2 for g in groups_of]
    home = [k for k in range(chunks) if 0 in CHUNK_Z[k]][0]
    home_q = CHUNK_Z[home].index(0)

    ep = lax.axis_index("ep")
    tp = lax.axis_index("tp")
    z, x = ep // nx, ep % nx
    y, c = tp // 2, tp % 2
    partner = y * 2 + (1 - c)
    y_up, y_dn, y_far = (y + 1) % NY, (y + NY - 1) % NY, (y + 2) % NY
    up, dn, far = y_up * 2 + c, y_dn * 2 + c, y_far * 2 + c

    hbm = (tok1_h, gain1_h, wq_h, wk_h, wv_h, sink_h, wo_h, tok2_h, gain2_h, routes_h, rw_h,
           wg_h, wu_h, wd_h, sg_h, su_h, sd_h, cosb_h, sinb_h, cosa_h, sina_h)
    vmem = (tok1, gain1, wq, wk, wv, sink, wo, tok2, gain2, routes, rw,
            wg, wu, wd, sg, su, sd, cosb, sinb, cosa, sina)
    vmem = vmem[:3] + (wkv.at[pl.ds(0, HEAD)], wkv.at[pl.ds(HEAD, HEAD)]) + vmem[5:]
    loads = [pltpu.make_async_copy(h, v, load_sem.at[i]) for i, (h, v) in enumerate(zip(hbm, vmem))]
    for i in (7, 8, 9, 10, 0, 1, 2, 3, 4, 5, 17, 18, 19, 20, 6, 14, 15, 16, 11, 12, 13):
        loads[i].start()

    barrier = pltpu.get_barrier_semaphore()
    for dz in range(nz):
        for dx in range(nx):
            if dz or dx:
                peer = ((z + dz) % nz) * nx + (x + dx) % nx
                pl.semaphore_signal(barrier, inc=1, device_id=(peer, tp), device_id_type=MESH)
    for step in range(1, n_tp):
        pl.semaphore_signal(barrier, inc=1, device_id=(ep, (tp + step) % n_tp), device_id_type=MESH)

    sends = []

    def send(src, dst, ssem, rsem, to_ep, to_tp):
        copy = pltpu.make_async_remote_copy(
            src_ref=src, dst_ref=dst, send_sem=ssem, recv_sem=rsem, device_id=(to_ep, to_tp), device_id_type=MESH
        )
        copy.start()
        sends.append((src, ssem))

    def arrived(dst, rsem):
        pltpu.make_async_copy(dst, dst, rsem).wait()

    with jax.named_scope("load_2"):
        for i in (7, 8, 9, 10):
            loads[i].wait()

    wide = tok2[...].astype(F32)
    scale = lax.rsqrt(jnp.mean(wide * wide, axis=-1, keepdims=True) + EPS)
    normed = (wide * scale * gain2[...]).astype(BF16)
    for j in range(n_tp):
        n2[j] = normed[:, j * f : (j + 1) * f]

    sub = lax.broadcasted_iota(jnp.int32, (128, t2), 0)
    named_t = jnp.zeros((128, t2), F32)
    weight_t = jnp.zeros((128, t2), F32)
    for k in range(topk):
        hit = sub == routes[k : k + 1]
        named_t = jnp.where(hit, 1.0, named_t)
        weight_t = jnp.where(hit, rw[k : k + 1], weight_t)
    row_i = lax.broadcasted_iota(jnp.int32, (t2, t2), 0)
    col_i = lax.broadcasted_iota(jnp.int32, (t2, t2), 1)
    before = jnp.where(row_i < col_i, 1.0, 0.0).astype(BF16)
    rank_t = jnp.dot(named_t.astype(BF16), before, preferred_element_type=F32)
    rank_t = jnp.where(named_t > 0.5, rank_t, -1.0)[: 2 * n_ep]
    cap_i = lax.broadcasted_iota(jnp.int32, (2 * n_ep, CAP, t2), 1).astype(F32)
    dispatch = jnp.where(rank_t[:, None, :] == cap_i, 1.0, 0.0).astype(BF16).reshape(2 * n_ep * CAP, t2)
    for far_one, column in enumerate((tp, far)):
        sent = jnp.dot(dispatch, n2[column], preferred_element_type=F32).astype(BF16)
        outgoing[far_one] = sent.reshape(n_ep, 2, CAP, f)

    def dispatch_all():
        with jax.named_scope("barrier"):
            pl.semaphore_wait(barrier, n_ep - 1 + n_tp - 1)
        send(kv.at[pl.ds(t1, BAND)], kv.at[pl.ds(0, BAND)], halo_s, halo_r, (ep + 1) % n_ep, tp)

        for far_one, column in enumerate((tp, far)):
            xs[home, column, home_q * nx + x] = outgoing[far_one, ep]
        for k, far_one in SEND_ORDER:
            for q, dz in enumerate(CHUNK_Z[k]):
                to_z = (z + nz - dz) % nz
                for i in range(nx):
                    if dz == 0 and i == 0:
                        continue
                    to = to_z * nx + (x + i) % nx
                    pltpu.make_async_remote_copy(
                        src_ref=outgoing.at[far_one, to], dst_ref=xs.at[k, (tp, far)[far_one], q * nx + x],
                        send_sem=dsp_s, recv_sem=dsp_r.at[k, far_one], device_id=(to, tp),
                        device_id_type=MESH,
                    ).start()

    per_z = 2 * nx * CAP

    def combine_weights():
        after = jnp.where(row_i > col_i, 1.0, 0.0).astype(BF16)
        named, weight = named_t.T, weight_t.T
        rank = jnp.dot(after, named.astype(BF16), preferred_element_type=F32)
        rank = jnp.where(named > 0.5, rank, -1.0).astype(BF16)
        w_hi = weight.astype(BF16)
        w_lo = (weight - w_hi.astype(F32)).astype(BF16)
        for zz in range(nz):
            e_row = lax.broadcasted_iota(jnp.int32, (128, per_z), 0)
            e_col = lax.broadcasted_iota(jnp.int32, (128, per_z), 1)
            spread = jnp.where(e_row == zz * 2 * nx + e_col // CAP, 1.0, 0.0).astype(BF16)
            slot = (lax.broadcasted_iota(jnp.int32, (t2, per_z), 1) % CAP).astype(F32)
            mine = jnp.dot(rank, spread, preferred_element_type=F32) == slot
            comb[zz, 0] = jnp.where(mine, jnp.dot(w_hi, spread, preferred_element_type=F32), 0.0).astype(BF16)
            comb[zz, 1] = jnp.where(mine, jnp.dot(w_lo, spread, preferred_element_type=F32), 0.0).astype(BF16)

    def halves(k):
        return pl.ds(0, slots_of[k] // 2), pl.ds(slots_of[k] // 2, slots_of[k] // 2)

    def dispatched(k, far_one):
        first = 1 if k == home else 0
        arrived(xs.at[k, 0, pl.ds(0, slots_of[k] - first)], dsp_r.at[k, far_one])

    def gather_start(k):
        dispatched(k, 0)
        own = xs.at[k, tp, pl.ds(0, slots_of[k])]
        send(own, own, ag_s.at[k, 0], ag_r.at[k, 0], ep, up)
        send(own, own, ag_s.at[k, 1], ag_r.at[k, 1], ep, dn)
        send(own, own, ag_s.at[k, 2], ag_r.at[k, 2], ep, partner)

    def gather_forward(k):
        low, high = halves(k)
        whole = pl.ds(0, slots_of[k])
        for i, (side, part, to) in enumerate(((dn, low, up), (up, high, dn))):
            got = xs.at[k, side, whole]
            arrived(got, ag_r.at[k, i])
            if k not in FAR_DIRECT:
                on = xs.at[k, side, part]
                send(on, on, ag_s.at[k, 3 + i], ag_r.at[k, 3 + i], ep, to)
            send(got, got, ag_s.at[k, 5 + i], ag_r.at[k, 5 + i], ep, partner)

    def gather_far(k):
        if k in FAR_DIRECT:
            dispatched(k, 1)
            got = xs.at[k, far, pl.ds(0, slots_of[k])]
            send(got, got, ag_s.at[k, 7], ag_r.at[k, 7], ep, partner)
            return
        for i, part in enumerate(halves(k)):
            got = xs.at[k, far, part]
            arrived(got, ag_r.at[k, 3 + i])
            send(got, got, ag_s.at[k, 7 + i], ag_r.at[k, 7 + i], ep, partner)

    def gather_end(k):
        other = 1 - c
        whole = pl.ds(0, slots_of[k])
        arrived(xs.at[k, partner, whole], ag_r.at[k, 2])
        arrived(xs.at[k, y_dn * 2 + other, whole], ag_r.at[k, 5])
        arrived(xs.at[k, y_up * 2 + other, whole], ag_r.at[k, 6])
        if k in FAR_DIRECT:
            arrived(xs.at[k, y_far * 2 + other, whole], ag_r.at[k, 7])
            return
        for i, part in enumerate(halves(k)):
            arrived(xs.at[k, y_far * 2 + other, part], ag_r.at[k, 7 + i])

    def pair_send(part, got, ss, rs, g):
        for o in (2, 1, 3, 0):
            t = (y + o) % NY
            send(part.at[t, 1 - c, pl.ds(0, g)], got.at[t, pl.ds(0, g)], ss.at[o], rs.at[o], ep, partner)

    def pair_sum(part, got, rs, o, g):
        t = (y + o) % NY
        at = pl.ds(0, g)
        arrived(got.at[t, at], rs.at[o])
        part[t, c, at] = (part[t, c, at].astype(F32) + got[t, at].astype(F32)).astype(BF16)

    def ring_first(part, got, far_in, near_in, ss, rs, h, g):
        pair_sum(part, got, rs, 2, g)
        pair_sum(part, got, rs, 1, g)
        send(part.at[y_far, c, pl.ds(0, h)], far_in.at[0, pl.ds(0, h)], ss.at[4], rs.at[4], ep, up)
        send(part.at[y_far, c, pl.ds(h, g - h)], far_in.at[1, pl.ds(0, g - h)], ss.at[5], rs.at[5], ep, dn)
        pair_sum(part, got, rs, 3, g)
        send(part.at[y_up, c, pl.ds(h, g - h)], near_in.at[0, pl.ds(h, g - h)], ss.at[6], rs.at[6], ep, up)
        pair_sum(part, got, rs, 0, g)
        send(part.at[y_dn, c, pl.ds(0, h)], near_in.at[1, pl.ds(0, h)], ss.at[7], rs.at[7], ep, dn)

    def ring_second(part, far_in, near_in, ss, rs, h, g):
        low, high = pl.ds(0, h), pl.ds(h, g - h)
        arrived(far_in.at[0, pl.ds(0, h)], rs.at[4])
        part[y_up, c, low] = (part[y_up, c, low].astype(F32) + far_in[0, pl.ds(0, h)].astype(F32)).astype(BF16)
        arrived(far_in.at[1, pl.ds(0, g - h)], rs.at[5])
        part[y_dn, c, high] = (part[y_dn, c, high].astype(F32) + far_in[1, pl.ds(0, g - h)].astype(F32)).astype(BF16)
        send(part.at[y_up, c, low], near_in.at[0, low], ss.at[8], rs.at[8], ep, up)
        send(part.at[y_dn, c, high], near_in.at[1, high], ss.at[9], rs.at[9], ep, dn)

    def ring_end(part, near_in, rs, h, g):
        low, high = pl.ds(0, h), pl.ds(h, g - h)
        arrived(near_in.at[0, high], rs.at[6])
        arrived(near_in.at[1, low], rs.at[7])
        arrived(near_in.at[0, low], rs.at[8])
        arrived(near_in.at[1, high], rs.at[9])
        at = pl.ds(0, g)
        return part[y, c, at].astype(F32) + near_in[0, at].astype(F32) + near_in[1, at].astype(F32)

    def experts(k):
        n_slots = slots_of[k]
        at = pl.ds(0, n_slots)

        def one(e, carry):
            rows = jnp.concatenate([xs[k, j, at, e].reshape(n_slots * CAP, f) for j in range(n_tp)], axis=1)
            gate = jnp.dot(rows, wg[e], preferred_element_type=F32)
            up_pre = jnp.dot(rows, wu[e], preferred_element_type=F32)
            hidden = (gate / (1.0 + jnp.exp(-gate)) * up_pre).astype(BF16)
            for j in range(n_tp):
                res = jnp.dot(hidden, wd[e, :, j * f : (j + 1) * f], preferred_element_type=F32).astype(BF16)
                p_ref[k, j // 2, j % 2, at, e] = res.reshape(n_slots, CAP, f)
            return carry

        lax.fori_loop(0, 2, one, 0)
        pair_send(p_ref.at[k], pr.at[k], rs_s.at[k], rs_r.at[k], groups_of[k])

    def rs_first(k):
        ring_first(p_ref.at[k], pr.at[k], r2.at[k], r1.at[k], rs_s.at[k], rs_r.at[k], half_of[k], groups_of[k])

    def rs_second(k):
        ring_second(p_ref.at[k], r2.at[k], r1.at[k], rs_s.at[k], rs_r.at[k], half_of[k], groups_of[k])

    def rs_end(k):
        total = ring_end(p_ref.at[k], r1.at[k], rs_r.at[k], half_of[k], groups_of[k])
        n_slots = slots_of[k]
        y_ref[k, pl.ds(0, n_slots)] = total.astype(BF16)
        if k == home:
            ret[z, x] = y_ref[k, home_q * nx + x]
        for q, dz in enumerate(CHUNK_Z[k]):
            src_z = (z + nz + dz) % nz
            for i in range(nx):
                if dz == 0 and i == 0:
                    continue
                xx = (x + i) % nx
                pltpu.make_async_remote_copy(
                    src_ref=y_ref.at[k, q * nx + xx], dst_ref=ret.at[z, x], send_sem=rt_s, recv_sem=rt_r.at[k],
                    device_id=(src_z * nx + xx, tp), device_id_type=MESH,
                ).start()

    def combine(k):
        first = 1 if k == home else 0
        arrived(y_ref.at[k, pl.ds(0, slots_of[k] - first)], rt_r.at[k])
        total = jnp.zeros((t2, f), F32)
        for dz in CHUNK_Z[k]:
            from_z = (z + nz - dz) % nz
            rows = ret[from_z].reshape(per_z, f)
            total += jnp.dot(comb[from_z, 0], rows, preferred_element_type=F32)
            total += jnp.dot(comb[from_z, 1], rows, preferred_element_type=F32)
        if k == 0:
            acc[...] = total
        else:
            acc[...] += total

    def shared():
        for i in (14, 15, 16):
            loads[i].wait()
        rows = jnp.concatenate([n2[j] for j in range(n_tp)], axis=1)
        gate = jnp.dot(rows, sg[...], preferred_element_type=F32)
        up_pre = jnp.dot(rows, su[...], preferred_element_type=F32)
        hidden = (gate / (1.0 + jnp.exp(-gate)) * up_pre).astype(BF16)
        for j in range(n_tp):
            res = jnp.dot(hidden, sd[:, j * f : (j + 1) * f], preferred_element_type=F32).astype(BF16)
            p_ref[chunks, j // 2, j % 2, pl.ds(0, groups_of[chunks])] = res.reshape(groups_of[chunks], 2, CAP, f)

    def shared_send():
        k = chunks
        pair_send(p_ref.at[k], pr.at[k], rs_s.at[k], rs_r.at[k], groups_of[k])

    def shared_end():
        k = chunks
        shr[...] = ring_end(p_ref.at[k], r1.at[k], rs_r.at[k], half_of[k], groups_of[k]).reshape(t2, f)

    blk = BAND
    n_blk = t1 // blk
    lane_b = lax.broadcasted_iota(jnp.int32, (blk, 128), 1)
    low_half = (lane_b % HEAD) < HEAD // 2
    is_key = lane_b < HEAD

    def project(i, carry):
        b = (i + n_blk - 1) % n_blk
        start = pl.multiple_of(b * blk, blk)

        def norm(r, inner):
            at = pl.ds(pl.multiple_of(r * 32, 32), 32)
            rows = tok1[pl.ds(pl.multiple_of(start + r * 32, 32), 32)].astype(F32)
            scl = lax.rsqrt(jnp.mean(rows * rows, axis=-1, keepdims=True) + EPS)
            nrm[at] = (rows * scl * gain1[...]).astype(BF16)
            return inner

        lax.fori_loop(0, blk // 32, norm, 0)
        at = pl.ds(start, blk)
        ca, sa = cosa[pl.ds(ep, 1)], sina[pl.ds(ep, 1)]
        cb, sb = cosb[at], sinb[at]
        cosine = ca * cb - sa * sb
        sine = sa * cb + ca * sb
        sine = jnp.where(low_half, -sine, sine)

        def turn(v, co, si):
            other = jnp.where(low_half, pltpu.roll(v, 128 - HEAD // 2, 1), pltpu.roll(v, HEAD // 2, 1))
            return v * co + other * si

        rows = nrm[...]
        qv = jnp.dot(rows, wq[...], preferred_element_type=F32)
        qs[at] = turn(qv, cosine, sine).astype(BF16)
        kvv = lax.dot_general(rows, wkv[...], (((1,), (1,)), ((), ())), preferred_element_type=F32)
        kv[pl.ds(pl.multiple_of(start + blk, blk), blk)] = turn(
            kvv, jnp.where(is_key, cosine, 1.0), jnp.where(is_key, sine, 0.0)
        ).astype(BF16)
        return carry

    def attend(b):
        keys = kv[pl.ds(b * blk, 2 * blk)]
        qb = qs[pl.ds(b * blk, blk)]
        zero = jnp.zeros_like(qb)
        q0 = jnp.where(is_key, qb, zero)
        q1 = jnp.where(is_key, pltpu.roll(qb.astype(F32), HEAD, 1).astype(BF16), zero)
        q_pos = lax.broadcasted_iota(jnp.int32, (blk, 2 * blk), 0) + blk
        k_pos = lax.broadcasted_iota(jnp.int32, (blk, 2 * blk), 1)
        gap = q_pos - k_pos
        seen = (gap >= 0) & (gap < BAND) & (k_pos + (ep * t1 + (b - 1) * blk) >= 0)
        outs = []
        for h, qh in enumerate((q0, q1)):
            s = lax.dot_general(qh, keys, (((1,), (1,)), ((), ())), preferred_element_type=F32) * HEAD**-0.5
            s = jnp.where(seen, s, -1e30)
            snk = sink[0:1, h : h + 1]
            peak = jnp.maximum(jnp.max(s, axis=-1, keepdims=True), snk)
            ex = jnp.where(seen, jnp.exp(s - peak), 0.0)
            den = jnp.sum(ex, axis=-1, keepdims=True) + jnp.exp(snk - peak)
            w = (ex / den).astype(BF16)
            outs.append(jnp.dot(w, keys, preferred_element_type=F32))
        att[pl.ds(b * blk, blk)] = jnp.where(is_key, pltpu.roll(outs[0], HEAD, 1), outs[1]).astype(BF16)

    def stage(name, fn, *operands):
        with jax.named_scope(name):
            return fn(*operands)

    def wait_loads(*which):
        for i in which:
            loads[i].wait()

    def project_first():
        wait_loads(0, 1, 2, 3, 4, 5, 17, 18, 19, 20)
        project(0, 0)

    def project_last():
        lax.fori_loop(1, n_blk, project, 0)

    def attend_rest(b, carry):
        attend(b)
        return carry

    def attend_later():
        lax.fori_loop(1, n_blk, attend_rest, 0)

    rows_tp = t1 // n_tp

    def attend_first():
        arrived(kv.at[pl.ds(0, blk)], halo_r)
        attend(0)
        for step in range(1, n_tp):
            to = (tp + step) % n_tp
            pltpu.make_async_remote_copy(
                src_ref=att.at[pl.ds(pl.multiple_of(to * rows_tp, rows_tp), rows_tp)], dst_ref=attx.at[tp],
                send_sem=at_s, recv_sem=at_r, device_id=(ep, to), device_id_type=MESH,
            ).start()
        attx[tp] = att[pl.ds(pl.multiple_of(tp * rows_tp, rows_tp), rows_tp)]

    x_up, x_dn, x_far = (x + 1) % nx, (x + nx - 1) % nx, (x + 2) % nx
    w_rows = 128 // nx
    w_half = w_rows // 2

    def weight_y_start():
        wait_loads(6)
        part = wo.at[pl.ds(pl.multiple_of(x * w_rows, w_rows), w_rows)]
        send(part, wof.at[x, c, y], wo_s.at[0], wo_r.at[0], ep, up)
        send(part, wof.at[x, c, y], wo_s.at[1], wo_r.at[1], ep, dn)
        wof[x, c, y] = wo[pl.ds(pl.multiple_of(x * w_rows, w_rows), w_rows)]

    def weight_y_forward():
        for i, (side, start, to) in enumerate(((y_dn, 0, up), (y_up, w_half, dn))):
            arrived(wof.at[x, c, side], wo_r.at[i])
            on = wof.at[x, c, side, pl.ds(start, w_half)]
            send(on, on, wo_s.at[2 + i], wo_r.at[2 + i], ep, to)

    def weight_x_start():
        for i, start in enumerate((0, w_half)):
            arrived(wof.at[x, c, y_far, pl.ds(start, w_half)], wo_r.at[2 + i])
        own = wof.at[x, c]
        send(own, own, wo_s.at[4], wo_r.at[4], z * nx + x_up, tp)
        send(own, own, wo_s.at[5], wo_r.at[5], z * nx + x_dn, tp)
        send(own, own, wo_s.at[8], wo_r.at[8], ep, partner)

    def weight_x_forward():
        for i, (side, start, to) in enumerate(((x_dn, 0, x_up), (x_up, NY // 2, x_dn))):
            got = wof.at[side, c]
            arrived(got, wo_r.at[4 + i])
            on = wof.at[side, c, pl.ds(start, NY // 2)]
            send(on, on, wo_s.at[6 + i], wo_r.at[6 + i], z * nx + to, tp)
            send(got, got, wo_s.at[9 + i], wo_r.at[9 + i], ep, partner)

    def weight_x_far():
        for i, start in enumerate((0, NY // 2)):
            got = wof.at[x_far, c, pl.ds(start, NY // 2)]
            arrived(got, wo_r.at[6 + i])
            send(got, got, wo_s.at[11 + i], wo_r.at[11 + i], ep, partner)

    def mixer_end():
        other = 1 - c
        arrived(wof.at[x, other], wo_r.at[8])
        arrived(wof.at[x_dn, other], wo_r.at[9])
        arrived(wof.at[x_up, other], wo_r.at[10])
        for i, start in enumerate((0, NY // 2)):
            arrived(wof.at[x_far, other, pl.ds(start, NY // 2)], wo_r.at[11 + i])
        arrived(attx.at[pl.ds(0, n_tp - 1)], at_r)
        rows = jnp.concatenate([attx[j] for j in range(n_tp)], axis=1)
        n_cols = 256

        def columns(n, carry):
            at = pl.ds(pl.multiple_of(n * n_cols, n_cols), n_cols)
            parts = [wof[q, j % 2, j // 2, :, at] for j in range(n_tp) for q in range(nx)]
            mix_o[:, at] = jnp.dot(rows, jnp.concatenate(parts, axis=0), preferred_element_type=F32).astype(BF16)
            return carry

        lax.fori_loop(0, d_model // n_cols, columns, 0)

    stage("project", project_first)
    stage("dispatch", dispatch_all)
    stage("w_y_start", weight_y_start)
    stage("project_last", project_last)
    stage("ag_start0", gather_start, 0)
    stage("shared", shared)
    stage("shared_send", shared_send)
    stage("w_y_fwd", weight_y_forward)
    stage("attend", attend_later)
    stage("ag_start1", gather_start, 1)
    stage("ag_fwd0", gather_forward, 0)
    stage("shared_first", rs_first, chunks)
    stage("ag_far0", gather_far, 0)
    stage("ag_start2", gather_start, 2)
    stage("shared_second", rs_second, chunks)
    stage("w_x_start", weight_x_start)
    stage("ag_fwd1", gather_forward, 1)
    stage("load_w", wait_loads, 11, 12, 13)
    stage("ag_end0", gather_end, 0)
    stage("experts0", experts, 0)
    stage("attend0", attend_first)
    stage("ag_start3", gather_start, 3)
    stage("ag_start4", gather_start, 4)
    stage("ag_far1", gather_far, 1)
    stage("ag_fwd2", gather_forward, 2)
    stage("rs_first0", rs_first, 0)
    stage("ag_end1", gather_end, 1)
    stage("experts1", experts, 1)
    stage("ag_fwd3", gather_forward, 3)
    stage("ag_fwd4", gather_forward, 4)
    stage("ag_far2", gather_far, 2)
    stage("rs_second0", rs_second, 0)
    stage("weights", combine_weights)
    stage("rs_first1", rs_first, 1)
    stage("ag_end2", gather_end, 2)
    stage("experts2", experts, 2)
    stage("rs_end0", rs_end, 0)
    stage("w_x_fwd", weight_x_forward)
    stage("ag_far3", gather_far, 3)
    stage("ag_far4", gather_far, 4)
    stage("rs_second1", rs_second, 1)
    stage("rs_first2", rs_first, 2)
    stage("ag_end3", gather_end, 3)
    stage("experts3", experts, 3)
    stage("rs_end1", rs_end, 1)
    stage("rs_second2", rs_second, 2)
    stage("rs_first3", rs_first, 3)
    stage("ag_end4", gather_end, 4)
    stage("experts4", experts, 4)
    stage("rs_end2", rs_end, 2)
    stage("rs_second3", rs_second, 3)
    stage("rs_first4", rs_first, 4)
    stage("shared_end", shared_end)
    stage("w_x_far", weight_x_far)
    stage("rs_end3", rs_end, 3)
    stage("rs_second4", rs_second, 4)
    stage("rs_end4", rs_end, 4)
    stage("mix_end", mixer_end)
    stage("combine0", combine, 0)
    stage("combine1", combine, 1)
    stage("combine2", combine, 2)
    stage("combine3", combine, 3)
    stage("combine4", combine, 4)

    def finish():
        moe_o[...] = (acc[...] + shr[...]).astype(BF16)
        for src, sem in sends:
            pltpu.make_async_copy(src, src, sem).wait()
        whole = outgoing.at[0, pl.ds(0, n_ep - 1)]
        sent_far = sum(slots_of[k] for k in FAR_DIRECT) - (1 if home in FAR_DIRECT else 0)
        pltpu.make_async_copy(whole, whole, dsp_s).wait()
        if sent_far:
            far_part = outgoing.at[1, pl.ds(0, sent_far)]
            pltpu.make_async_copy(far_part, far_part, dsp_s).wait()
        pltpu.make_async_copy(whole, whole, rt_s).wait()
        rows_out = attx.at[pl.ds(0, n_tp - 1)]
        pltpu.make_async_copy(rows_out, rows_out, at_s).wait()

    stage("finish", finish)


def build(mesh, nx=NX):
    n_ep = mesh.shape["ep"]
    n_tp = mesh.shape["tp"]
    nz = n_ep // nx

    def local(tok1, gain1, wq, wk, wv, sink, wo, tok2, gain2, routes, rw, wg, wu, wd, sg, su, sd):
        t1, d_model = tok1.shape
        t2, topk = routes.shape
        eff = wg.shape[2]
        sff = sg.shape[1]
        f = d_model // n_tp
        chunks = len(CHUNK_Z)
        slot_groups = nx * max(len(c) for c in CHUNK_Z)
        groups = max(slot_groups, t2 // (2 * CAP))
        half = (groups + 1) // 2
        rows_tp = t1 // n_tp
        tables = tuple(jnp.asarray(t) for t in rope_tables(t1, n_ep))
        args = (
            tok1, gain1.reshape(1, -1), wq, wk.T, wv.T, sink.reshape(1, -1), wo, tok2, gain2.reshape(1, -1), routes.T, rw.T,
            wg, wu, wd, sg, su, sd, *tables,
        )
        vm = pltpu.VMEM
        dma = pltpu.SemaphoreType.DMA
        scratch = [vm((8, 128) if i in (3, 4) else a.shape, a.dtype) for i, a in enumerate(args)] + [
            vm((n_tp, t2, f), BF16),
                vm((nz, 2, t2, 2 * nx * CAP), BF16),
            vm((2, n_ep, 2, CAP, f), BF16),
            vm((chunks, n_tp, slot_groups, 2, CAP, f), BF16),
            vm((BAND, d_model), BF16),
            vm((t1, 128), BF16),
            vm((t1 + BAND, 128), BF16),
            vm((128, d_model), BF16),
            vm((nx, 2, NY, 128 // nx, d_model), BF16),
            vm((t1, 128), BF16),
            vm((n_tp, rows_tp, 128), BF16),
            vm((chunks + 1, NY, 2, groups, 2, CAP, f), BF16),
            vm((chunks + 1, NY, groups, 2, CAP, f), BF16),
            vm((chunks + 1, 2, half, 2, CAP, f), BF16),
            vm((chunks + 1, 2, groups, 2, CAP, f), BF16),
            vm((chunks, slot_groups, 2, CAP, f), BF16),
            vm((nz, nx, 2, CAP, f), BF16),
            vm((t2, f), F32),
            vm((t2, f), F32),
            dma((len(args),)),
            dma, dma,
            dma, dma((chunks, 2)),
            dma((chunks, 9)), dma((chunks, 9)),
            dma((chunks + 1, 10)), dma((chunks + 1, 10)),
            dma((13,)), dma((13,)),
            dma, dma,
            dma, dma((chunks,)),
        ]
        cfg = (nz, nx, n_tp, d_model, t1, t2, topk, eff, sff)
        return pl.pallas_call(
            functools.partial(kernel, cfg),
            name="whole",
            out_shape=(
                jax.ShapeDtypeStruct((rows_tp, d_model), BF16),
                jax.ShapeDtypeStruct((t2, f), BF16),
            ),
            in_specs=[pl.BlockSpec(memory_space=pltpu.HBM)] * len(args),
            out_specs=(pl.BlockSpec(memory_space=pltpu.VMEM),) * 2,
            scratch_shapes=scratch,
            compiler_params=pltpu.CompilerParams(
                collective_id=0, has_side_effects=True, vmem_limit_bytes=44 * 1024 * 1024
            ),
        )(*[pltpu.with_memory_space_constraint(a, pltpu.HBM) for a in args])
    in_specs = (
        P("ep", None), P(), P(None, "tp"), P(None, "tp"), P(None, "tp"), P("tp"), P("tp", None),
        P("ep", None), P(), P("ep", None), P("ep", None),
        P("ep", None, "tp"), P("ep", None, "tp"), P("ep", "tp", None),
        P(None, "tp"), P(None, "tp"), P("tp", None),
    )
    out_specs = (P(("ep", "tp"), None), P("ep", "tp"))
    return jax.shard_map(local, mesh=mesh, in_specs=in_specs, out_specs=out_specs, check_vma=False)


def solution(mesh):
    return build(mesh)
```

```python
import functools

import jax
import jax.numpy as jnp
import numpy as np
from jax import lax
from jax.experimental import pallas as pl
from jax.experimental.pallas import tpu as pltpu
from jax.sharding import PartitionSpec as P

HEAD = 64
BAND = 128
CAP = 16
NX = 4
NY = 4
ROPE_BASE = 10000.0
EPS = 1e-06
MESH = pl.DeviceIdType.MESH
F32 = jnp.float32
BF16 = jnp.bfloat16


CHUNK_Z = ((0, 1), (4, -2), (3, -3), (2,), (-1,))
FAR_DIRECT = (0, 2, 3, 4)
SEND_ORDER = ((0, 0), (0, 1), (1, 0), (2, 0), (3, 0), (4, 0), (2, 1), (3, 1), (4, 1))


def rope_tables(rows, n_ep):
    freqs = ROPE_BASE ** (-np.arange(0, HEAD, 2, dtype=np.float64) / HEAD)
    lanes = np.tile(freqs, 4)[None, :]
    within = np.arange(rows, dtype=np.float64)[:, None] * lanes
    starts = np.arange(n_ep, dtype=np.float64)[:, None] * rows * lanes
    return tuple(
        np.asarray(t, np.float32) for t in (np.cos(within), np.sin(within), np.cos(starts), np.sin(starts))
    )


def kernel(cfg, *refs):
    nz, nx, n_tp, d_model, t1, t2, topk, eff, sff = cfg
    n_in = 21
    (
        tok1_h, gain1_h, wq_h, wk_h, wv_h, sink_h, wo_h, tok2_h, gain2_h, routes_h, rw_h,
        wg_h, wu_h, wd_h, sg_h, su_h, sd_h, cosb_h, sinb_h, cosa_h, sina_h,
    ) = refs[:n_in]
    mix_o, moe_o = refs[n_in : n_in + 2]
    (
        tok1, gain1, wq, wk, wv, sink, wo, tok2, gain2, routes, rw,
        wg, wu, wd, sg, su, sd, cosb, sinb, cosa, sina,
    ) = refs[n_in + 2 : 2 * n_in + 2]
    (
        n2, comb, outgoing, xs, nrm, qs, kv, wkv, wof, att, attx, p_ref, pr, r2, r1, y_ref, ret, shr,
        acc,
        load_sem, halo_s, halo_r, dsp_s, dsp_r, ag_s, ag_r, rs_s, rs_r, wo_s, wo_r, at_s, at_r, rt_s, rt_r,
    ) = refs[2 * n_in + 2 :]
    f = d_model // n_tp
    n_ep = nz * nx
    chunks = len(CHUNK_Z)
    slots_of = [nx * len(c) for c in CHUNK_Z]
    groups_of = slots_of + [t2 // (2 * CAP)]
    half_of = [g // 2 for g in groups_of]
    home = [k for k in range(chunks) if 0 in CHUNK_Z[k]][0]
    home_q = CHUNK_Z[home].index(0)

    ep = lax.axis_index("ep")
    tp = lax.axis_index("tp")
    z, x = ep // nx, ep % nx
    y, c = tp // 2, tp % 2
    partner = y * 2 + (1 - c)
    y_up, y_dn, y_far = (y + 1) % NY, (y + NY - 1) % NY, (y + 2) % NY
    up, dn, far = y_up * 2 + c, y_dn * 2 + c, y_far * 2 + c

    hbm = (tok1_h, gain1_h, wq_h, wk_h, wv_h, sink_h, wo_h, tok2_h, gain2_h, routes_h, rw_h,
           wg_h, wu_h, wd_h, sg_h, su_h, sd_h, cosb_h, sinb_h, cosa_h, sina_h)
    vmem = (tok1, gain1, wq, wk, wv, sink, wo, tok2, gain2, routes, rw,
            wg, wu, wd, sg, su, sd, cosb, sinb, cosa, sina)
    vmem = vmem[:3] + (wkv.at[pl.ds(0, HEAD)], wkv.at[pl.ds(HEAD, HEAD)]) + vmem[5:]
    loads = [pltpu.make_async_copy(h, v, load_sem.at[i]) for i, (h, v) in enumerate(zip(hbm, vmem))]
    for i in (7, 8, 9, 10, 0, 1, 2, 3, 4, 5, 17, 18, 19, 20, 6, 14, 15, 16, 11, 12, 13):
        loads[i].start()

    barrier = pltpu.get_barrier_semaphore()
    for dz in range(nz):
        for dx in range(nx):
            if dz or dx:
                peer = ((z + dz) % nz) * nx + (x + dx) % nx
                pl.semaphore_signal(barrier, inc=1, device_id=(peer, tp), device_id_type=MESH)
    for step in range(1, n_tp):
        pl.semaphore_signal(barrier, inc=1, device_id=(ep, (tp + step) % n_tp), device_id_type=MESH)

    sends = []

    def send(src, dst, ssem, rsem, to_ep, to_tp):
        copy = pltpu.make_async_remote_copy(
            src_ref=src, dst_ref=dst, send_sem=ssem, recv_sem=rsem, device_id=(to_ep, to_tp), device_id_type=MESH
        )
        copy.start()
        sends.append((src, ssem))

    def arrived(dst, rsem):
        pltpu.make_async_copy(dst, dst, rsem).wait()

    with jax.named_scope("load_2"):
        for i in (7, 8, 9, 10):
            loads[i].wait()

    wide = tok2[...].astype(F32)
    scale = lax.rsqrt(jnp.mean(wide * wide, axis=-1, keepdims=True) + EPS)
    normed = (wide * scale * gain2[...]).astype(BF16)
    for j in range(n_tp):
        n2[j] = normed[:, j * f : (j + 1) * f]

    sub = lax.broadcasted_iota(jnp.int32, (128, t2), 0)
    named_t = jnp.zeros((128, t2), F32)
    weight_t = jnp.zeros((128, t2), F32)
    for k in range(topk):
        hit = sub == routes[k : k + 1]
        named_t = jnp.where(hit, 1.0, named_t)
        weight_t = jnp.where(hit, rw[k : k + 1], weight_t)
    row_i = lax.broadcasted_iota(jnp.int32, (t2, t2), 0)
    col_i = lax.broadcasted_iota(jnp.int32, (t2, t2), 1)
    before = jnp.where(row_i < col_i, 1.0, 0.0).astype(BF16)
    rank_t = jnp.dot(named_t.astype(BF16), before, preferred_element_type=F32)
    rank_t = jnp.where(named_t > 0.5, rank_t, -1.0)[: 2 * n_ep]
    cap_i = lax.broadcasted_iota(jnp.int32, (2 * n_ep, CAP, t2), 1).astype(F32)
    dispatch = jnp.where(rank_t[:, None, :] == cap_i, 1.0, 0.0).astype(BF16).reshape(2 * n_ep * CAP, t2)
    for far_one, column in enumerate((tp, far)):
        sent = jnp.dot(dispatch, n2[column], preferred_element_type=F32).astype(BF16)
        outgoing[far_one] = sent.reshape(n_ep, 2, CAP, f)

    def dispatch_all():
        with jax.named_scope("barrier"):
            pl.semaphore_wait(barrier, n_ep - 1 + n_tp - 1)
        send(kv.at[pl.ds(t1, BAND)], kv.at[pl.ds(0, BAND)], halo_s, halo_r, (ep + 1) % n_ep, tp)

        for far_one, column in enumerate((tp, far)):
            xs[home, column, home_q * nx + x] = outgoing[far_one, ep]
        for k, far_one in SEND_ORDER:
            for q, dz in enumerate(CHUNK_Z[k]):
                to_z = (z + nz - dz) % nz
                for i in range(nx):
                    if dz == 0 and i == 0:
                        continue
                    to = to_z * nx + (x + i) % nx
                    pltpu.make_async_remote_copy(
                        src_ref=outgoing.at[far_one, to], dst_ref=xs.at[k, (tp, far)[far_one], q * nx + x],
                        send_sem=dsp_s, recv_sem=dsp_r.at[k, far_one], device_id=(to, tp),
                        device_id_type=MESH,
                    ).start()

    per_z = 2 * nx * CAP

    def combine_weights():
        after = jnp.where(row_i > col_i, 1.0, 0.0).astype(BF16)
        named, weight = named_t.T, weight_t.T
        rank = jnp.dot(after, named.astype(BF16), preferred_element_type=F32)
        rank = jnp.where(named > 0.5, rank, -1.0).astype(BF16)
        w_hi = weight.astype(BF16)
        w_lo = (weight - w_hi.astype(F32)).astype(BF16)
        for zz in range(nz):
            e_row = lax.broadcasted_iota(jnp.int32, (128, per_z), 0)
            e_col = lax.broadcasted_iota(jnp.int32, (128, per_z), 1)
            spread = jnp.where(e_row == zz * 2 * nx + e_col // CAP, 1.0, 0.0).astype(BF16)
            slot = (lax.broadcasted_iota(jnp.int32, (t2, per_z), 1) % CAP).astype(F32)
            mine = jnp.dot(rank, spread, preferred_element_type=F32) == slot
            comb[zz, 0] = jnp.where(mine, jnp.dot(w_hi, spread, preferred_element_type=F32), 0.0).astype(BF16)
            comb[zz, 1] = jnp.where(mine, jnp.dot(w_lo, spread, preferred_element_type=F32), 0.0).astype(BF16)

    def halves(k):
        return pl.ds(0, slots_of[k] // 2), pl.ds(slots_of[k] // 2, slots_of[k] // 2)

    def dispatched(k, far_one):
        first = 1 if k == home else 0
        arrived(xs.at[k, 0, pl.ds(0, slots_of[k] - first)], dsp_r.at[k, far_one])

    def gather_start(k):
        dispatched(k, 0)
        own = xs.at[k, tp, pl.ds(0, slots_of[k])]
        send(own, own, ag_s.at[k, 0], ag_r.at[k, 0], ep, up)
        send(own, own, ag_s.at[k, 1], ag_r.at[k, 1], ep, dn)
        send(own, own, ag_s.at[k, 2], ag_r.at[k, 2], ep, partner)

    def gather_forward(k):
        low, high = halves(k)
        whole = pl.ds(0, slots_of[k])
        for i, (side, part, to) in enumerate(((dn, low, up), (up, high, dn))):
            got = xs.at[k, side, whole]
            arrived(got, ag_r.at[k, i])
            if k not in FAR_DIRECT:
                on = xs.at[k, side, part]
                send(on, on, ag_s.at[k, 3 + i], ag_r.at[k, 3 + i], ep, to)
            send(got, got, ag_s.at[k, 5 + i], ag_r.at[k, 5 + i], ep, partner)

    def gather_far(k):
        if k in FAR_DIRECT:
            dispatched(k, 1)
            got = xs.at[k, far, pl.ds(0, slots_of[k])]
            send(got, got, ag_s.at[k, 7], ag_r.at[k, 7], ep, partner)
            return
        for i, part in enumerate(halves(k)):
            got = xs.at[k, far, part]
            arrived(got, ag_r.at[k, 3 + i])
            send(got, got, ag_s.at[k, 7 + i], ag_r.at[k, 7 + i], ep, partner)

    def gather_end(k):
        other = 1 - c
        whole = pl.ds(0, slots_of[k])
        arrived(xs.at[k, partner, whole], ag_r.at[k, 2])
        arrived(xs.at[k, y_dn * 2 + other, whole], ag_r.at[k, 5])
        arrived(xs.at[k, y_up * 2 + other, whole], ag_r.at[k, 6])
        if k in FAR_DIRECT:
            arrived(xs.at[k, y_far * 2 + other, whole], ag_r.at[k, 7])
            return
        for i, part in enumerate(halves(k)):
            arrived(xs.at[k, y_far * 2 + other, part], ag_r.at[k, 7 + i])

    def pair_send(part, got, ss, rs, g):
        for o in (2, 1, 3, 0):
            t = (y + o) % NY
            send(part.at[t, 1 - c, pl.ds(0, g)], got.at[t, pl.ds(0, g)], ss.at[o], rs.at[o], ep, partner)

    def pair_sum(part, got, rs, o, g):
        t = (y + o) % NY
        at = pl.ds(0, g)
        arrived(got.at[t, at], rs.at[o])
        part[t, c, at] = (part[t, c, at].astype(F32) + got[t, at].astype(F32)).astype(BF16)

    def ring_first(part, got, far_in, near_in, ss, rs, h, g):
        pair_sum(part, got, rs, 2, g)
        pair_sum(part, got, rs, 1, g)
        send(part.at[y_far, c, pl.ds(0, h)], far_in.at[0, pl.ds(0, h)], ss.at[4], rs.at[4], ep, up)
        send(part.at[y_far, c, pl.ds(h, g - h)], far_in.at[1, pl.ds(0, g - h)], ss.at[5], rs.at[5], ep, dn)
        pair_sum(part, got, rs, 3, g)
        send(part.at[y_up, c, pl.ds(h, g - h)], near_in.at[0, pl.ds(h, g - h)], ss.at[6], rs.at[6], ep, up)
        pair_sum(part, got, rs, 0, g)
        send(part.at[y_dn, c, pl.ds(0, h)], near_in.at[1, pl.ds(0, h)], ss.at[7], rs.at[7], ep, dn)

    def ring_second(part, far_in, near_in, ss, rs, h, g):
        low, high = pl.ds(0, h), pl.ds(h, g - h)
        arrived(far_in.at[0, pl.ds(0, h)], rs.at[4])
        part[y_up, c, low] = (part[y_up, c, low].astype(F32) + far_in[0, pl.ds(0, h)].astype(F32)).astype(BF16)
        arrived(far_in.at[1, pl.ds(0, g - h)], rs.at[5])
        part[y_dn, c, high] = (part[y_dn, c, high].astype(F32) + far_in[1, pl.ds(0, g - h)].astype(F32)).astype(BF16)
        send(part.at[y_up, c, low], near_in.at[0, low], ss.at[8], rs.at[8], ep, up)
        send(part.at[y_dn, c, high], near_in.at[1, high], ss.at[9], rs.at[9], ep, dn)

    def ring_end(part, near_in, rs, h, g):
        low, high = pl.ds(0, h), pl.ds(h, g - h)
        arrived(near_in.at[0, high], rs.at[6])
        arrived(near_in.at[1, low], rs.at[7])
        arrived(near_in.at[0, low], rs.at[8])
        arrived(near_in.at[1, high], rs.at[9])
        at = pl.ds(0, g)
        return part[y, c, at].astype(F32) + near_in[0, at].astype(F32) + near_in[1, at].astype(F32)

    def experts(k):
        n_slots = slots_of[k]
        at = pl.ds(0, n_slots)

        def one(e, carry):
            rows = jnp.concatenate([xs[k, j, at, e].reshape(n_slots * CAP, f) for j in range(n_tp)], axis=1)
            gate = jnp.dot(rows, wg[e], preferred_element_type=F32)
            up_pre = jnp.dot(rows, wu[e], preferred_element_type=F32)
            hidden = (gate / (1.0 + jnp.exp(-gate)) * up_pre).astype(BF16)
            for j in range(n_tp):
                res = jnp.dot(hidden, wd[e, :, j * f : (j + 1) * f], preferred_element_type=F32).astype(BF16)
                p_ref[k, j // 2, j % 2, at, e] = res.reshape(n_slots, CAP, f)
            return carry

        lax.fori_loop(0, 2, one, 0)
        pair_send(p_ref.at[k], pr.at[k], rs_s.at[k], rs_r.at[k], groups_of[k])

    def rs_first(k):
        ring_first(p_ref.at[k], pr.at[k], r2.at[k], r1.at[k], rs_s.at[k], rs_r.at[k], half_of[k], groups_of[k])

    def rs_second(k):
        ring_second(p_ref.at[k], r2.at[k], r1.at[k], rs_s.at[k], rs_r.at[k], half_of[k], groups_of[k])

    def rs_end(k):
        total = ring_end(p_ref.at[k], r1.at[k], rs_r.at[k], half_of[k], groups_of[k])
        n_slots = slots_of[k]
        y_ref[k, pl.ds(0, n_slots)] = total.astype(BF16)
        if k == home:
            ret[z, x] = y_ref[k, home_q * nx + x]
        for q, dz in enumerate(CHUNK_Z[k]):
            src_z = (z + nz + dz) % nz
            for i in range(nx):
                if dz == 0 and i == 0:
                    continue
                xx = (x + i) % nx
                pltpu.make_async_remote_copy(
                    src_ref=y_ref.at[k, q * nx + xx], dst_ref=ret.at[z, x], send_sem=rt_s, recv_sem=rt_r.at[k],
                    device_id=(src_z * nx + xx, tp), device_id_type=MESH,
                ).start()

    def combine(k):
        first = 1 if k == home else 0
        arrived(y_ref.at[k, pl.ds(0, slots_of[k] - first)], rt_r.at[k])
        total = jnp.zeros((t2, f), F32)
        for dz in CHUNK_Z[k]:
            from_z = (z + nz - dz) % nz
            rows = ret[from_z].reshape(per_z, f)
            total += jnp.dot(comb[from_z, 0], rows, preferred_element_type=F32)
            total += jnp.dot(comb[from_z, 1], rows, preferred_element_type=F32)
        if k == 0:
            acc[...] = total
        else:
            acc[...] += total

    def shared():
        for i in (14, 15, 16):
            loads[i].wait()
        rows = jnp.concatenate([n2[j] for j in range(n_tp)], axis=1)
        gate = jnp.dot(rows, sg[...], preferred_element_type=F32)
        up_pre = jnp.dot(rows, su[...], preferred_element_type=F32)
        hidden = (gate / (1.0 + jnp.exp(-gate)) * up_pre).astype(BF16)
        for j in range(n_tp):
            res = jnp.dot(hidden, sd[:, j * f : (j + 1) * f], preferred_element_type=F32).astype(BF16)
            p_ref[chunks, j // 2, j % 2, pl.ds(0, groups_of[chunks])] = res.reshape(groups_of[chunks], 2, CAP, f)

    def shared_send():
        k = chunks
        pair_send(p_ref.at[k], pr.at[k], rs_s.at[k], rs_r.at[k], groups_of[k])

    def shared_end():
        k = chunks
        shr[...] = ring_end(p_ref.at[k], r1.at[k], rs_r.at[k], half_of[k], groups_of[k]).reshape(t2, f)

    blk = BAND
    n_blk = t1 // blk
    lane_b = lax.broadcasted_iota(jnp.int32, (blk, 128), 1)
    low_half = (lane_b % HEAD) < HEAD // 2
    is_key = lane_b < HEAD

    def project(i, carry):
        b = (i + n_blk - 1) % n_blk
        start = pl.multiple_of(b * blk, blk)

        def norm(r, inner):
            at = pl.ds(pl.multiple_of(r * 32, 32), 32)
            rows = tok1[pl.ds(pl.multiple_of(start + r * 32, 32), 32)].astype(F32)
            scl = lax.rsqrt(jnp.mean(rows * rows, axis=-1, keepdims=True) + EPS)
            nrm[at] = (rows * scl * gain1[...]).astype(BF16)
            return inner

        lax.fori_loop(0, blk // 32, norm, 0)
        at = pl.ds(start, blk)
        ca, sa = cosa[pl.ds(ep, 1)], sina[pl.ds(ep, 1)]
        cb, sb = cosb[at], sinb[at]
        cosine = ca * cb - sa * sb
        sine = sa * cb + ca * sb
        sine = jnp.where(low_half, -sine, sine)

        def turn(v, co, si):
            other = jnp.where(low_half, pltpu.roll(v, 128 - HEAD // 2, 1), pltpu.roll(v, HEAD // 2, 1))
            return v * co + other * si

        rows = nrm[...]
        qv = jnp.dot(rows, wq[...], preferred_element_type=F32)
        qs[at] = turn(qv, cosine, sine).astype(BF16)
        kvv = lax.dot_general(rows, wkv[...], (((1,), (1,)), ((), ())), preferred_element_type=F32)
        kv[pl.ds(pl.multiple_of(start + blk, blk), blk)] = turn(
            kvv, jnp.where(is_key, cosine, 1.0), jnp.where(is_key, sine, 0.0)
        ).astype(BF16)
        return carry

    def attend(b):
        keys = kv[pl.ds(b * blk, 2 * blk)]
        qb = qs[pl.ds(b * blk, blk)]
        zero = jnp.zeros_like(qb)
        q0 = jnp.where(is_key, qb, zero)
        q1 = jnp.where(is_key, pltpu.roll(qb.astype(F32), HEAD, 1).astype(BF16), zero)
        q_pos = lax.broadcasted_iota(jnp.int32, (blk, 2 * blk), 0) + blk
        k_pos = lax.broadcasted_iota(jnp.int32, (blk, 2 * blk), 1)
        gap = q_pos - k_pos
        seen = (gap >= 0) & (gap < BAND) & (k_pos + (ep * t1 + (b - 1) * blk) >= 0)
        outs = []
        for h, qh in enumerate((q0, q1)):
            s = lax.dot_general(qh, keys, (((1,), (1,)), ((), ())), preferred_element_type=F32) * HEAD**-0.5
            s = jnp.where(seen, s, -1e30)
            snk = sink[0:1, h : h + 1]
            peak = jnp.maximum(jnp.max(s, axis=-1, keepdims=True), snk)
            ex = jnp.where(seen, jnp.exp(s - peak), 0.0)
            den = jnp.sum(ex, axis=-1, keepdims=True) + jnp.exp(snk - peak)
            w = (ex / den).astype(BF16)
            outs.append(jnp.dot(w, keys, preferred_element_type=F32))
        att[pl.ds(b * blk, blk)] = jnp.where(is_key, pltpu.roll(outs[0], HEAD, 1), outs[1]).astype(BF16)

    def stage(name, fn, *operands):
        with jax.named_scope(name):
            return fn(*operands)

    def wait_loads(*which):
        for i in which:
            loads[i].wait()

    def project_first():
        wait_loads(0, 1, 2, 3, 4, 5, 17, 18, 19, 20)
        project(0, 0)

    def project_last():
        lax.fori_loop(1, n_blk, project, 0)

    def attend_rest(b, carry):
        attend(b)
        return carry

    def attend_later():
        lax.fori_loop(1, n_blk, attend_rest, 0)

    rows_tp = t1 // n_tp

    def attend_first():
        arrived(kv.at[pl.ds(0, blk)], halo_r)
        attend(0)
        for step in range(1, n_tp):
            to = (tp + step) % n_tp
            pltpu.make_async_remote_copy(
                src_ref=att.at[pl.ds(pl.multiple_of(to * rows_tp, rows_tp), rows_tp)], dst_ref=attx.at[tp],
                send_sem=at_s, recv_sem=at_r, device_id=(ep, to), device_id_type=MESH,
            ).start()
        attx[tp] = att[pl.ds(pl.multiple_of(tp * rows_tp, rows_tp), rows_tp)]

    x_up, x_dn, x_far = (x + 1) % nx, (x + nx - 1) % nx, (x + 2) % nx
    w_rows = 128 // nx
    w_half = w_rows // 2

    def weight_y_start():
        wait_loads(6)
        part = wo.at[pl.ds(pl.multiple_of(x * w_rows, w_rows), w_rows)]
        send(part, wof.at[x, c, y], wo_s.at[0], wo_r.at[0], ep, up)
        send(part, wof.at[x, c, y], wo_s.at[1], wo_r.at[1], ep, dn)
        wof[x, c, y] = wo[pl.ds(pl.multiple_of(x * w_rows, w_rows), w_rows)]

    def weight_y_forward():
        for i, (side, start, to) in enumerate(((y_dn, 0, up), (y_up, w_half, dn))):
            arrived(wof.at[x, c, side], wo_r.at[i])
            on = wof.at[x, c, side, pl.ds(start, w_half)]
            send(on, on, wo_s.at[2 + i], wo_r.at[2 + i], ep, to)

    def weight_x_start():
        for i, start in enumerate((0, w_half)):
            arrived(wof.at[x, c, y_far, pl.ds(start, w_half)], wo_r.at[2 + i])
        own = wof.at[x, c]
        send(own, own, wo_s.at[4], wo_r.at[4], z * nx + x_up, tp)
        send(own, own, wo_s.at[5], wo_r.at[5], z * nx + x_dn, tp)
        send(own, own, wo_s.at[8], wo_r.at[8], ep, partner)

    def weight_x_forward():
        for i, (side, start, to) in enumerate(((x_dn, 0, x_up), (x_up, NY // 2, x_dn))):
            got = wof.at[side, c]
            arrived(got, wo_r.at[4 + i])
            on = wof.at[side, c, pl.ds(start, NY // 2)]
            send(on, on, wo_s.at[6 + i], wo_r.at[6 + i], z * nx + to, tp)
            send(got, got, wo_s.at[9 + i], wo_r.at[9 + i], ep, partner)

    def weight_x_far():
        for i, start in enumerate((0, NY // 2)):
            got = wof.at[x_far, c, pl.ds(start, NY // 2)]
            arrived(got, wo_r.at[6 + i])
            send(got, got, wo_s.at[11 + i], wo_r.at[11 + i], ep, partner)

    def mixer_end():
        other = 1 - c
        arrived(wof.at[x, other], wo_r.at[8])
        arrived(wof.at[x_dn, other], wo_r.at[9])
        arrived(wof.at[x_up, other], wo_r.at[10])
        for i, start in enumerate((0, NY // 2)):
            arrived(wof.at[x_far, other, pl.ds(start, NY // 2)], wo_r.at[11 + i])
        arrived(attx.at[pl.ds(0, n_tp - 1)], at_r)
        rows = jnp.concatenate([attx[j] for j in range(n_tp)], axis=1)
        n_cols = 256

        def columns(n, carry):
            at = pl.ds(pl.multiple_of(n * n_cols, n_cols), n_cols)
            parts = [wof[q, j % 2, j // 2, :, at] for j in range(n_tp) for q in range(nx)]
            mix_o[:, at] = jnp.dot(rows, jnp.concatenate(parts, axis=0), preferred_element_type=F32).astype(BF16)
            return carry

        lax.fori_loop(0, d_model // n_cols, columns, 0)

    stage("project", project_first)
    stage("dispatch", dispatch_all)
    stage("w_y_start", weight_y_start)
    stage("project_last", project_last)
    stage("ag_start0", gather_start, 0)
    stage("shared", shared)
    stage("shared_send", shared_send)
    stage("w_y_fwd", weight_y_forward)
    stage("attend", attend_later)
    stage("ag_start1", gather_start, 1)
    stage("ag_fwd0", gather_forward, 0)
    stage("shared_first", rs_first, chunks)
    stage("ag_far0", gather_far, 0)
    stage("ag_start2", gather_start, 2)
    stage("shared_second", rs_second, chunks)
    stage("ag_fwd1", gather_forward, 1)
    stage("load_w", wait_loads, 11, 12, 13)
    stage("ag_end0", gather_end, 0)
    stage("experts0", experts, 0)
    stage("w_x_start", weight_x_start)
    stage("attend0", attend_first)
    stage("weights", combine_weights)
    stage("ag_start3", gather_start, 3)
    stage("ag_start4", gather_start, 4)
    stage("rs_first0", rs_first, 0)
    stage("ag_far1", gather_far, 1)
    stage("ag_fwd2", gather_forward, 2)
    stage("ag_end1", gather_end, 1)
    stage("experts1", experts, 1)
    stage("ag_fwd3", gather_forward, 3)
    stage("ag_fwd4", gather_forward, 4)
    stage("ag_far2", gather_far, 2)
    stage("rs_second0", rs_second, 0)
    stage("rs_first1", rs_first, 1)
    stage("ag_end2", gather_end, 2)
    stage("experts2", experts, 2)
    stage("rs_end0", rs_end, 0)
    stage("ag_far3", gather_far, 3)
    stage("ag_far4", gather_far, 4)
    stage("rs_second1", rs_second, 1)
    stage("rs_first2", rs_first, 2)
    stage("ag_end3", gather_end, 3)
    stage("experts3", experts, 3)
    stage("ag_end4", gather_end, 4)
    stage("experts4", experts, 4)
    stage("w_x_fwd", weight_x_forward)
    stage("rs_end1", rs_end, 1)
    stage("rs_second2", rs_second, 2)
    stage("rs_first3", rs_first, 3)
    stage("rs_first4", rs_first, 4)
    stage("rs_end2", rs_end, 2)
    stage("rs_second3", rs_second, 3)
    stage("rs_second4", rs_second, 4)
    stage("shared_end", shared_end)
    stage("rs_end3", rs_end, 3)
    stage("w_x_far", weight_x_far)
    stage("rs_end4", rs_end, 4)
    stage("mix_end", mixer_end)
    stage("combine0", combine, 0)
    stage("combine1", combine, 1)
    stage("combine2", combine, 2)
    stage("combine3", combine, 3)
    stage("combine4", combine, 4)

    def finish():
        moe_o[...] = (acc[...] + shr[...]).astype(BF16)
        for src, sem in sends:
            pltpu.make_async_copy(src, src, sem).wait()
        whole = outgoing.at[0, pl.ds(0, n_ep - 1)]
        sent_far = sum(slots_of[k] for k in FAR_DIRECT) - (1 if home in FAR_DIRECT else 0)
        pltpu.make_async_copy(whole, whole, dsp_s).wait()
        if sent_far:
            far_part = outgoing.at[1, pl.ds(0, sent_far)]
            pltpu.make_async_copy(far_part, far_part, dsp_s).wait()
        pltpu.make_async_copy(whole, whole, rt_s).wait()
        rows_out = attx.at[pl.ds(0, n_tp - 1)]
        pltpu.make_async_copy(rows_out, rows_out, at_s).wait()

    stage("finish", finish)


def build(mesh, nx=NX):
    n_ep = mesh.shape["ep"]
    n_tp = mesh.shape["tp"]
    nz = n_ep // nx

    def local(tok1, gain1, wq, wk, wv, sink, wo, tok2, gain2, routes, rw, wg, wu, wd, sg, su, sd):
        t1, d_model = tok1.shape
        t2, topk = routes.shape
        eff = wg.shape[2]
        sff = sg.shape[1]
        f = d_model // n_tp
        chunks = len(CHUNK_Z)
        slot_groups = nx * max(len(c) for c in CHUNK_Z)
        groups = max(slot_groups, t2 // (2 * CAP))
        half = (groups + 1) // 2
        rows_tp = t1 // n_tp
        tables = tuple(jnp.asarray(t) for t in rope_tables(t1, n_ep))
        args = (
            tok1, gain1.reshape(1, -1), wq, wk.T, wv.T, sink.reshape(1, -1), wo, tok2, gain2.reshape(1, -1), routes.T, rw.T,
            wg, wu, wd, sg, su, sd, *tables,
        )
        vm = pltpu.VMEM
        dma = pltpu.SemaphoreType.DMA
        scratch = [vm((8, 128) if i in (3, 4) else a.shape, a.dtype) for i, a in enumerate(args)] + [
            vm((n_tp, t2, f), BF16),
                vm((nz, 2, t2, 2 * nx * CAP), BF16),
            vm((2, n_ep, 2, CAP, f), BF16),
            vm((chunks, n_tp, slot_groups, 2, CAP, f), BF16),
            vm((BAND, d_model), BF16),
            vm((t1, 128), BF16),
            vm((t1 + BAND, 128), BF16),
            vm((128, d_model), BF16),
            vm((nx, 2, NY, 128 // nx, d_model), BF16),
            vm((t1, 128), BF16),
            vm((n_tp, rows_tp, 128), BF16),
            vm((chunks + 1, NY, 2, groups, 2, CAP, f), BF16),
            vm((chunks + 1, NY, groups, 2, CAP, f), BF16),
            vm((chunks + 1, 2, half, 2, CAP, f), BF16),
            vm((chunks + 1, 2, groups, 2, CAP, f), BF16),
            vm((chunks, slot_groups, 2, CAP, f), BF16),
            vm((nz, nx, 2, CAP, f), BF16),
            vm((t2, f), F32),
            vm((t2, f), F32),
            dma((len(args),)),
            dma, dma,
            dma, dma((chunks, 2)),
            dma((chunks, 9)), dma((chunks, 9)),
            dma((chunks + 1, 10)), dma((chunks + 1, 10)),
            dma((13,)), dma((13,)),
            dma, dma,
            dma, dma((chunks,)),
        ]
        cfg = (nz, nx, n_tp, d_model, t1, t2, topk, eff, sff)
        return pl.pallas_call(
            functools.partial(kernel, cfg),
            name="whole",
            out_shape=(
                jax.ShapeDtypeStruct((rows_tp, d_model), BF16),
                jax.ShapeDtypeStruct((t2, f), BF16),
            ),
            in_specs=[pl.BlockSpec(memory_space=pltpu.HBM)] * len(args),
            out_specs=(pl.BlockSpec(memory_space=pltpu.VMEM),) * 2,
            scratch_shapes=scratch,
            compiler_params=pltpu.CompilerParams(
                collective_id=0, has_side_effects=True, vmem_limit_bytes=44 * 1024 * 1024
            ),
        )(*[pltpu.with_memory_space_constraint(a, pltpu.HBM) for a in args])
    in_specs = (
        P("ep", None), P(), P(None, "tp"), P(None, "tp"), P(None, "tp"), P("tp"), P("tp", None),
        P("ep", None), P(), P("ep", None), P("ep", None),
        P("ep", None, "tp"), P("ep", None, "tp"), P("ep", "tp", None),
        P(None, "tp"), P(None, "tp"), P("tp", None),
    )
    out_specs = (P(("ep", "tp"), None), P("ep", "tp"))
    return jax.shard_map(local, mesh=mesh, in_specs=in_specs, out_specs=out_specs, check_vma=False)


def solution(mesh):
    return build(mesh)
```
